32 devices in a mesh: ep: 8 (over z, core), tp: 4 (over y, x).
Axes of the slice: x: 2, y: 2, z: 4, core: 2. Of those that a mesh axis runs over, the one named last changes fastest.
Arguments:
- query_pairs: bfloat16 [3072, 2048], P('ep', 'tp'), may hold values from -64 to 64
- key_pairs: bfloat16 [3072, 2048], P('ep', 'tp'), may hold values from -64 to 64
- value_rows: bfloat16 [3072, 2048], P('ep', 'tp'), may hold values from -6 to 6
- head_lambda: float32 [16], P('tp'), may hold values from 0.3 to 0.8
- head_gain: float32 [128], replicated, may hold values from 0.1 to 1.9
- out_weight: bfloat16 [2048, 2048], P('tp'), may hold values from -0.1875 to 0.1875
- moe_input: bfloat16 [1280, 2048], P('ep'), may hold values from -6 to 6
- ffn_gain: float32 [2048], replicated, may hold values from 0.1 to 1.9
- routes: int32 [1280, 2], P('ep'), may hold values from 0 to 7, all different within a row; in each aligned block of 160 rows (0 to 159, 160 to 319, ...) at most 50 rows name the same one
- route_weight: float32 [1280, 2], P('ep'), may hold values from 0.25 to 2.5
- gate_weight: bfloat16 [8, 2048, 2048], P('ep', None, 'tp'), may hold values from -0.125 to 0.125
- up_weight: bfloat16 [8, 2048, 2048], P('ep', None, 'tp'), may hold values from -0.125 to 0.125
- down_weight: bfloat16 [8, 2048, 2048], P('ep', 'tp'), may hold values from -0.1875 to 0.1875
- shared_gate: bfloat16 [2048, 2048], P(None, 'tp'), may hold values from -0.125 to 0.125
- shared_up: bfloat16 [2048, 2048], P(None, 'tp'), may hold values from -0.125 to 0.125
- shared_down: bfloat16 [2048, 2048], P('tp'), may hold values from -0.1875 to 0.1875
Outputs:
- attn_out: bfloat16 [3072, 2048], P('ep', 'tp')
- moe_out: bfloat16 [1280, 2048], P('ep', 'tp')
The draws below stay inside these ranges and needn't reach their ends.
Inputs may be any that keep to these rules, and one draw needn't show every extreme that they name: `routes`: in each aligned block of 160 rows (the rows of one device along ep) no expert is named more than 50 times, a bound that some block reaches; a row names 2 different experts.
All inputs are finite; a program needn't handle non-finite values.
Results may differ from the reference program's by a relative error of at most 0.017.
The reference program's roundings to bfloat16 on the way count: a program that leaves them out, or rounds other values in their place, can miss the bound.
Values may be sent and summed in bfloat16 or wider, within the bound.
A program may use at most 64 MiB of HBM per device.

```python
import math
import jax
import jax.numpy as jnp
import numpy as np
from jax import lax

D = 2048
HEADS = 16
HEAD = 64
VHEAD = 128
FF = 2048
SFF = 2048
TOP_K = 2
KEY_BLOCK = 128
TOK_B = 160
TOKENS_A = 3072
TOKENS_B = 1280
EXPERTS = 8
CAP = 50
N_TP = 4


def paired_draw(key):
    draw_shape = (TOKENS_A, HEADS, 2, HEAD)
    queries = 1.3 * jax.random.truncated_normal(jax.random.fold_in(key, 101), -4.0, 4.0, draw_shape, jnp.float32)
    keyset = 1.3 * jax.random.truncated_normal(jax.random.fold_in(key, 102), -4.0, 4.0, draw_shape, jnp.float32)
    return (jnp.clip(queries, -64.0, 64.0), jnp.clip(keyset, -64.0, 64.0))


def draw_query_pairs(key, part):
    return paired_draw(key)[0].reshape(TOKENS_A, HEADS * 2 * HEAD).astype(jnp.bfloat16)


def draw_key_pairs(key, part):
    return paired_draw(key)[1].reshape(TOKENS_A, HEADS * 2 * HEAD).astype(jnp.bfloat16)


def with_spikes(entries, rng, source, target, blocks, factor):
    owner, partner = [(jnp.arange(entries.shape[axis_at]) // (entries.shape[axis_at] // blocks)).reshape([-1 if axis == axis_at else 1 for axis in range(entries.ndim)]) for axis_at in (source, target)]
    chosen = jax.random.permutation(rng, blocks)[partner]
    strong = (owner == chosen) | (owner == (partner + blocks // 2) % blocks)
    return jnp.where(strong, factor * entries, entries)


def level_of(key, dims, split, smallest, high):
    level, own = 1.0, jax.random.fold_in(key, 6)
    for dim, parts in split:
        draws = jnp.exp(jax.random.uniform(jax.random.fold_in(own, dim), (parts,), jnp.float32, smallest / len(split), high / len(split)))
        level = level * jnp.repeat(draws, dims[dim] // parts).reshape([-1 if axis == dim else 1 for axis in range(len(dims))])
    return level


def routed_block(own_key, own, number, rows, count, top, limit, lean):
    order = jax.random.permutation(own_key, count)
    heavy_load, usual = portions_of(count, rows * top, limit, lean, True), portions_of(count, rows * top, limit, lean, False)
    places = jnp.arange(count)

    def named(tallies, turn):
        used = int((tallies > 0).sum())
        fixed = max(1, used // 4)
        passed = fixed + (places - fixed + turn * (used - fixed)) % max(1, count - fixed)
        return jnp.zeros((count,), jnp.int32).at[order[jnp.where(places < fixed, places, passed)]].set(jnp.asarray(tallies, jnp.int32))

    tallies = jnp.where(number % 4 == 0, named(heavy_load, number // 4), named(usual, number - number // 4 - 1))
    mixed = jax.random.permutation(jax.random.fold_in(own, 3), count)
    source_of, taker = mixed[0:count // 2 * 2:2], mixed[1:count // 2 * 2:2]
    slack = jnp.minimum(tallies[source_of] - 1, limit - tallies[taker]) // 2
    slack = jnp.where((source_of == order[0]) | (taker == order[0]) | (tallies[taker] == 0), 0, jnp.maximum(slack, 0))
    passed = jax.random.randint(jax.random.fold_in(own, 4), (count // 2,), 0, 1 << 20) % (slack + 1)
    tallies = tallies.at[source_of].add(-passed).at[taker].add(passed)
    labels = jnp.searchsorted(jnp.cumsum(tallies), jnp.arange(rows * top), side="right").astype(jnp.int32)
    grid = labels.reshape(top, rows).T
    grid = grid[jax.random.permutation(jax.random.fold_in(own, 1), rows)]
    turn = jax.random.randint(jax.random.fold_in(own, 2), (rows, 1), 0, top)
    return jnp.take_along_axis(grid, (jnp.arange(top)[None, :] + turn) % top, axis=1)


def portions_of(number_of, total, limit, slope, full):
    weights = [(1 << 20) // math.isqrt(standing ** slope) + 1 for standing in range(1, number_of + 1)]
    largest = limit if full else min(limit, max(-(-total // number_of), total * weights[0] // sum(weights)))
    least = 1 if total - largest >= number_of - 1 else 0
    counts, spare = [largest] + [least] * (number_of - 1), total - largest - least * (number_of - 1)
    while spare > 0:
        free = [i for i in range(1, number_of) if counts[i] < largest] or [i for i in range(1, number_of) if counts[i] < limit]
        mass, remaining = sum([weights[i] for i in free]), spare
        for i in free:
            more = min(limit - counts[i], max(1, remaining * weights[i] // mass), spare)
            counts[i] = counts[i] + more
            spare = spare - more
    return np.array(counts)


def scatter_about(rng, dims, scale, bound, shards=(), held_as=jnp.bfloat16):
    loudness = level_of(rng, dims, shards, -0.22, 0.18) if shards else 1.0
    drawn = jax.random.normal(rng, dims, jnp.float32) * scale * loudness
    return jnp.minimum(jnp.maximum(drawn, -bound), bound).astype(held_as)


def bell_draw_with(stream_key, shape, width, limit, shards, heavy, kind=jnp.bfloat16):
    values = width * jax.random.normal(stream_key, shape, jnp.float32)
    if shards:
        values = values * level_of(stream_key, shape, shards, -0.22, 0.18)
    return jnp.clip(with_spikes(values, jax.random.fold_in(stream_key, 3), *heavy), -limit, limit).astype(kind)


def setup_inputs(seed: int = 0) -> dict:
    streams_of = jax.random.split(jax.random.key(seed), 17)
    query_pairs = draw_query_pairs(jax.random.fold_in(streams_of[16], 71), 0)
    key_pairs = draw_key_pairs(jax.random.fold_in(streams_of[16], 71), 0)
    value_rows = scatter_about(streams_of[2], (TOKENS_A, HEADS * VHEAD), 1.0, 6.0, ((0, 8), (1, 4)))
    head_lambda = jnp.clip(0.3 + 0.5 * jax.random.uniform(streams_of[3], (HEADS,), jnp.float32) ** level_of(streams_of[3], (HEADS,), ((0, 4),), -0.2, 0.2), 0.3, 0.8)
    head_gain = jnp.clip(1.0 + 0.18 * jax.random.normal(streams_of[4], (VHEAD,), jnp.float32), 0.1, 1.9)
    out_weight = bell_draw_with(streams_of[5], (HEADS * VHEAD, D), (HEADS * VHEAD) ** -0.5, 0.1875, ((0, 4),), (0, 1, 4, 2.0))
    moe_input = scatter_about(streams_of[6], (TOKENS_B, D), 1.0, 6.0, ((0, 8),))
    ffn_gain = jnp.clip(1.0 + 0.18 * jax.random.normal(streams_of[7], (D,), jnp.float32), 0.1, 1.9)
    routes_keys = jax.random.split(jax.random.fold_in(streams_of[8], 1), TOKENS_B // TOK_B)
    routes_turns = jax.random.permutation(jax.random.fold_in(streams_of[8], 3), TOKENS_B // TOK_B)
    routes = jax.vmap(lambda own, number: routed_block(jax.random.fold_in(streams_of[8], 2), own, number, TOK_B, EXPERTS, TOP_K, CAP, 1))(routes_keys, routes_turns).reshape((TOKENS_B, TOP_K))
    route_weight = jnp.clip(jnp.exp(math.log(2.5) - 2.3025851 * jax.random.uniform(streams_of[9], (TOKENS_B, TOP_K), jnp.float32) ** level_of(streams_of[9], (TOKENS_B, TOP_K), ((0, 8),), -0.2, 0.2)), 0.25, 2.5)
    gate_weight = scatter_about(streams_of[10], (EXPERTS, D, FF), D ** -0.5, 0.125, ((0, 8), (2, 4)))
    up_weight = scatter_about(streams_of[11], (EXPERTS, D, FF), D ** -0.5, 0.125, ((0, 8), (2, 4)))
    down_weight = bell_draw_with(streams_of[12], (EXPERTS, FF, D), FF ** -0.5, 0.1875, ((0, 8), (1, 4)), (1, 2, 4, 2.0))
    shared_gate = scatter_about(streams_of[13], (D, SFF), D ** -0.5, 0.125, ((1, 4),))
    shared_up = scatter_about(streams_of[14], (D, SFF), D ** -0.5, 0.125, ((1, 4),))
    shared_down = bell_draw_with(streams_of[15], (SFF, D), SFF ** -0.5, 0.1875, ((0, 4),), (0, 1, 4, 2.0))
    return {"query_pairs": query_pairs, "key_pairs": key_pairs, "value_rows": value_rows, "head_lambda": head_lambda, "head_gain": head_gain, "out_weight": out_weight, "moe_input": moe_input, "ffn_gain": ffn_gain, "routes": routes, "route_weight": route_weight, "gate_weight": gate_weight, "up_weight": up_weight, "down_weight": down_weight, "shared_gate": shared_gate, "shared_up": shared_up, "shared_down": shared_down}


theta_base = 500000.0
norm_eps = 1e-06
masked_low = -1e+30

def rotate(inputs, positions):
    half_size = inputs.shape[-1] // 2
    frequency = theta_base ** (-(jnp.arange(half_size, dtype=jnp.float32) * 2.0) / inputs.shape[-1])
    angles = positions.astype(jnp.float32)[:, None] * frequency[None, :]
    cosine = jnp.cos(angles)[:, None, None, :]
    sine_part = jnp.sin(angles)[:, None, None, :]
    front_half = inputs[..., :half_size]
    back_half = inputs[..., half_size:]
    return jnp.concatenate([front_half * cosine - back_half * sine_part, back_half * cosine + front_half * sine_part], axis=-1)

def attention(query_pairs, key_pairs, value_rows, head_lambda, head_gain, out_weight):
    total_rows = query_pairs.shape[0]
    head_count = head_lambda.shape[0]
    head_size = query_pairs.shape[1] // (2 * head_count)
    value_size = value_rows.shape[1] // head_count
    positions = jnp.arange(total_rows, dtype=jnp.int32)
    rot_queries = rotate(query_pairs.astype(jnp.float32).reshape(total_rows, head_count, 2, head_size), positions).astype(jnp.bfloat16)
    rot_keys = rotate(key_pairs.astype(jnp.float32).reshape(total_rows, head_count, 2, head_size), positions).astype(jnp.bfloat16)
    key_blocks = total_rows // KEY_BLOCK
    block_keys = rot_keys.reshape(key_blocks, KEY_BLOCK, head_count, 2, head_size).astype(jnp.float32)
    block_values = value_rows.reshape(key_blocks, KEY_BLOCK, head_count, value_size).astype(jnp.float32)
    key_positions = positions.reshape(key_blocks, KEY_BLOCK)
    query_block = math.gcd(total_rows, 256)
    query_count = total_rows // query_block

    def one_block(inputs):
        block_queries, query_positions = inputs
        scores = jnp.einsum('qhmd,bkhmd->hmqbk', block_queries.astype(jnp.float32), block_keys) * head_size ** (-0.5)
        allowed = key_positions[None, :, :] <= query_positions[:, None, None]
        scores = jnp.where(allowed, scores, masked_low)
        block_max = lax.optimization_barrier(jnp.max(scores, axis=-1))
        weights = jnp.where(allowed, jnp.exp(scores - block_max[..., None]), 0.0)
        block_sum = lax.optimization_barrier(jnp.sum(weights, axis=-1))
        rounded = lax.optimization_barrier(weights.astype(jnp.bfloat16)).astype(jnp.float32)
        block_out = jnp.einsum('hmqbk,bkhc->hmqbc', rounded, block_values)
        row_max = lax.optimization_barrier(jnp.max(block_max, axis=-1, keepdims=True))
        rescale = jnp.exp(block_max - row_max)
        summed = lax.optimization_barrier(jnp.sum(rescale * block_sum, axis=-1))
        combined = lax.optimization_barrier(jnp.sum(rescale[..., None] * block_out, axis=-2))
        return combined / summed[..., None]
    outputs = lax.map(one_block, (rot_queries.reshape(query_count, query_block, head_count, 2, head_size), positions.reshape(query_count, query_block)))
    difference = outputs[:, :, 0] - head_lambda[None, :, None, None] * outputs[:, :, 1]
    inverse_rms = lax.rsqrt(lax.optimization_barrier(jnp.mean(difference * difference, axis=-1, keepdims=True)) + norm_eps)
    normed = (difference * inverse_rms * head_gain.astype(jnp.float32)).astype(jnp.bfloat16)
    normed = normed.transpose(0, 2, 1, 3).reshape(total_rows, head_count * value_size)
    group_cols = head_count * value_size // N_TP
    grouped = normed.reshape(total_rows, N_TP, group_cols).transpose(1, 0, 2)
    weight_groups = out_weight.reshape(N_TP, group_cols, out_weight.shape[1])

    def add_group(running, block_parts):
        partial_out = jnp.dot(block_parts[0], block_parts[1], preferred_element_type=jnp.float32)
        return (running + lax.optimization_barrier(partial_out.astype(jnp.bfloat16)).astype(jnp.float32), None)
    result, _ = lax.scan(add_group, jnp.zeros((total_rows, out_weight.shape[1]), jnp.float32), (grouped, weight_groups))
    return result.astype(jnp.bfloat16)

def swiglu_blocks(inputs, gate_w, up_w, down_w):
    model_width = gate_w.shape[0]
    block_width = gate_w.shape[1] // N_TP
    gate_blocks = gate_w.reshape(model_width, N_TP, block_width).transpose(1, 0, 2)
    up_blocks = up_w.reshape(model_width, N_TP, block_width).transpose(1, 0, 2)
    down_blocks = down_w.reshape(N_TP, block_width, down_w.shape[1])

    def add_block(running, block_parts):
        gate_part = jnp.dot(inputs, block_parts[0], preferred_element_type=jnp.float32)
        up_part = jnp.dot(inputs, block_parts[1], preferred_element_type=jnp.float32)
        hidden = (jax.nn.silu(gate_part) * up_part).astype(jnp.bfloat16)
        partial_out = jnp.dot(hidden, block_parts[2], preferred_element_type=jnp.float32)
        return (running + lax.optimization_barrier(partial_out.astype(jnp.bfloat16)).astype(jnp.float32), None)
    result, _ = lax.scan(add_block, jnp.zeros((inputs.shape[0], down_w.shape[1]), jnp.float32), (gate_blocks, up_blocks, down_blocks))
    return result

def mixture(moe_input, ffn_gain, routes, route_weight, gate_weight, up_weight, down_weight, shared_gate, shared_up, shared_down):
    row_values = moe_input.astype(jnp.float32)
    inverse_rms = lax.rsqrt(lax.optimization_barrier(jnp.mean(row_values * row_values, axis=-1, keepdims=True)) + norm_eps)
    normed = (row_values * inverse_rms * ffn_gain.astype(jnp.float32)).astype(jnp.bfloat16)
    total_rows = normed.shape[0]
    experts = gate_weight.shape[0]
    blocks = total_rows // TOK_B
    flat_routes = routes.reshape(blocks, TOK_B * TOP_K)
    onehot = (flat_routes[..., None] == jnp.arange(experts, dtype=jnp.int32)).astype(jnp.int32)
    slot_rank = lax.optimization_barrier(jnp.sum((jnp.cumsum(onehot, axis=1) - 1) * onehot, axis=-1)).astype(jnp.int32)
    token_ids = jnp.arange(blocks, dtype=jnp.int32)[:, None] * TOK_B + jnp.arange(TOK_B * TOP_K, dtype=jnp.int32)[None, :] // TOP_K
    source_ids = jnp.broadcast_to(jnp.arange(blocks, dtype=jnp.int32)[:, None], flat_routes.shape)
    slot_table = jnp.full((experts, blocks, CAP), total_rows, jnp.int32).at[flat_routes, source_ids, slot_rank].set(token_ids)
    padded = jnp.concatenate([normed, jnp.zeros((1, normed.shape[1]), jnp.bfloat16)], axis=0)

    def one_expert(inputs):
        chosen = padded[inputs[0].reshape(-1)]
        return swiglu_blocks(chosen, inputs[1], inputs[2], inputs[3]).astype(jnp.bfloat16)
    expert_out = lax.map(one_expert, (slot_table, gate_weight, up_weight, down_weight))
    expert_out = expert_out.reshape(experts, blocks, CAP, normed.shape[1])
    block_index = (jnp.arange(total_rows, dtype=jnp.int32) // TOK_B)[:, None]
    picked = expert_out[routes, block_index, slot_rank.reshape(total_rows, TOP_K)]
    shared_sum = swiglu_blocks(normed, shared_gate, shared_up, shared_down)
    combined = lax.optimization_barrier(jnp.sum(route_weight[..., None] * picked.astype(jnp.float32), axis=1)) + shared_sum
    return combined.astype(jnp.bfloat16)

def reference(query_pairs, key_pairs, value_rows, head_lambda, head_gain, out_weight, moe_input, ffn_gain, routes, route_weight, gate_weight, up_weight, down_weight, shared_gate, shared_up, shared_down):
    attn_out = attention(query_pairs, key_pairs, value_rows, head_lambda, head_gain, out_weight)
    moe_out = mixture(moe_input, ffn_gain, routes, route_weight, gate_weight, up_weight, down_weight, shared_gate, shared_up, shared_down)
    return (attn_out, moe_out)
```

```python
import functools

import jax
import jax.numpy as jnp
from jax import lax
from jax.experimental import pallas as pl
from jax.experimental.pallas import tpu as pltpu
from jax.sharding import PartitionSpec as P

TOP_K = 2
KEY_BLOCK = 128


theta_base = 500000.0
norm_eps = 1e-06
masked_low = -1e30


def rotate(inputs, positions):
    half_size = inputs.shape[-1] // 2
    frequency = theta_base ** (-(jnp.arange(half_size, dtype=jnp.float32) * 2.0) / inputs.shape[-1])
    angles = positions.astype(jnp.float32)[:, None] * frequency[None, :]
    cosine = jnp.cos(angles)[:, None, None, :]
    sine_part = jnp.sin(angles)[:, None, None, :]
    front_half = inputs[..., :half_size]
    back_half = inputs[..., half_size:]
    return jnp.concatenate(
        [front_half * cosine - back_half * sine_part, back_half * cosine + front_half * sine_part],
        axis=-1,
    )


def generic_attention(query_pairs, key_pairs, value_rows, head_lambda, head_gain, out_weight):
    local_rows = query_pairs.shape[0]
    local_heads = head_lambda.shape[0]
    head_size = query_pairs.shape[1] // (2 * local_heads)
    value_size = value_rows.shape[1] // local_heads
    positions = lax.axis_index("ep") * local_rows + jnp.arange(local_rows, dtype=jnp.int32)
    rot_queries = rotate(
        query_pairs.astype(jnp.float32).reshape(local_rows, local_heads, 2, head_size), positions
    ).astype(jnp.bfloat16)
    rot_keys = rotate(
        key_pairs.astype(jnp.float32).reshape(local_rows, local_heads, 2, head_size), positions
    ).astype(jnp.bfloat16)
    rot_keys = rot_keys.reshape(local_rows, local_heads * 2 * head_size)
    zero_init = (
        jnp.full((local_heads, 2, local_rows), masked_low, jnp.float32),
        jnp.zeros((local_heads, 2, local_rows), jnp.float32),
        jnp.zeros((local_heads, 2, local_rows, value_size), jnp.float32),
    )
    piece_keys = lax.all_gather(rot_keys, "ep", axis=0, tiled=True)
    piece_values = lax.all_gather(value_rows, "ep", axis=0, tiled=True)
    block_count = piece_keys.shape[0] // KEY_BLOCK
    group_size = 4
    group_count = block_count // group_size
    grouped_keys = piece_keys.reshape(group_count, group_size, KEY_BLOCK, local_heads, 2, head_size)
    grouped_values = piece_values.reshape(
        group_count, group_size, KEY_BLOCK, local_heads, value_size
    )

    def one_group(current, inputs):
        block_keys, block_values, group_index = inputs
        key_positions = group_index * group_size * KEY_BLOCK + jnp.arange(
            group_size * KEY_BLOCK, dtype=jnp.int32
        ).reshape(group_size, KEY_BLOCK)
        scores = jnp.einsum(
            "qhmd,gkhmd->hmqgk", rot_queries, block_keys, preferred_element_type=jnp.float32
        ) * head_size ** (-0.5)
        allowed = key_positions[None, :, :] <= positions[:, None, None]
        scores = jnp.where(allowed, scores, masked_low)
        block_max = jnp.max(scores, axis=-1)
        weights = jnp.where(allowed, jnp.exp(scores - block_max[..., None]), 0.0)
        block_sum = jnp.sum(weights, axis=-1)
        block_out = jnp.einsum(
            "hmqgk,gkhc->hmqgc",
            weights.astype(jnp.bfloat16),
            block_values,
            preferred_element_type=jnp.float32,
        )
        run_max, run_sum, run_out = current
        new_max = jnp.maximum(run_max, jnp.max(block_max, axis=-1))
        old_scale = jnp.exp(run_max - new_max)
        new_scale = jnp.exp(block_max - new_max[..., None])
        run_sum = run_sum * old_scale + jnp.sum(new_scale * block_sum, axis=-1)
        run_out = run_out * old_scale[..., None] + jnp.sum(
            new_scale[..., None] * block_out, axis=-2
        )
        return ((new_max, run_sum, run_out), None)

    result, _ = lax.scan(
        one_group,
        zero_init,
        (grouped_keys, grouped_values, jnp.arange(group_count, dtype=jnp.int32)),
    )
    run_max, run_sum, run_out = result
    map_outputs = run_out / run_sum[..., None]
    difference = map_outputs[:, 0] - head_lambda[:, None, None] * map_outputs[:, 1]
    inverse_rms = lax.rsqrt(jnp.mean(difference * difference, axis=-1, keepdims=True) + norm_eps)
    normed_heads = (difference * inverse_rms * head_gain).astype(jnp.bfloat16)
    head_rows = normed_heads.transpose(1, 0, 2).reshape(local_rows, local_heads * value_size)
    mixer_terms = jnp.dot(head_rows, out_weight, preferred_element_type=jnp.float32)
    attn_out = lax.psum_scatter(
        mixer_terms.astype(jnp.bfloat16), "tp", scatter_dimension=1, tiled=True
    )
    return attn_out


MESH = pl.DeviceIdType.MESH
f32, bf16 = jnp.float32, jnp.bfloat16


def rotate_kernel(head_size, scale, q_ref, k_ref, cos_ref, sin_ref, rq_ref, rk_ref):
    heads, _, width = rq_ref.shape
    half = head_size // 2
    lane = lax.broadcasted_iota(jnp.int32, (q_ref.shape[0], width), 1)
    front = lane % head_size < half
    cosine, sine = cos_ref[...], sin_ref[...]
    for source, target, factor in ((q_ref, rq_ref, scale), (k_ref, rk_ref, 1.0)):
        for h in range(heads):
            x = source[:, h * width : (h + 1) * width].astype(f32)
            partner = jnp.where(front, pltpu.roll(x, width - half, 1), pltpu.roll(x, half, 1))
            turned = (x * cosine + partner * sine).astype(bf16)
            target[h] = turned if factor == 1.0 else turned * jnp.asarray(factor, bf16)


def attention_kernel(
    n, heads, lam_ref, gain_ref, rq_ref, rk_ref, v_ref, w_ref, out_ref,
    q_buf, k_buf, v_buf, vt_buf, hn_send, hn_buf, w_buf, acc, m_buf, l_buf,
    q_ss, q_rs, k_ss, k_rs, v_ss, v_rs, fk_ss, fk_rs, fv_ss, fv_rs, h_ss, h_rs, loc, w_sem,
):
    me = lax.axis_index("ep")
    g = n // heads
    my_head, my_core = me // g, me % g
    rows = rk_ref.shape[1]
    sub = rows // g
    width = rk_ref.shape[2]
    vw = v_buf.shape[2]

    barrier = pltpu.get_barrier_semaphore()
    for step in range(1, n):
        pl.semaphore_signal(barrier, inc=1, device_id={"ep": lax.rem(me + step, n)}, device_id_type=MESH)
    w_copy = pltpu.make_async_copy(w_ref, w_buf, w_sem)
    w_copy.start()

    def q_src(dest):
        start = pl.multiple_of(((dest % g + me) % g) * sub, sub)
        return rq_ref.at[dest // g, pl.ds(start, sub), :]

    def v_src(dest):
        return v_ref.at[:, pl.ds(pl.multiple_of((dest // g) * vw, vw), vw)]

    own = (
        pltpu.make_async_copy(q_src(me), q_buf.at[me], loc.at[0]),
        pltpu.make_async_copy(rk_ref.at[my_head], k_buf.at[me], loc.at[1]),
        pltpu.make_async_copy(v_src(me), v_buf.at[me], loc.at[2]),
    )
    for copy in own:
        copy.start()
    pl.semaphore_wait(barrier, n - 1)

    def q_copy(dest):
        return pltpu.make_async_remote_copy(
            q_src(dest), q_buf.at[me], q_ss.at[dest], q_rs.at[me],
            device_id={"ep": dest}, device_id_type=MESH)

    def k_copy(dest):
        return pltpu.make_async_remote_copy(
            rk_ref.at[dest // g], k_buf.at[me], k_ss.at[dest], k_rs.at[me],
            device_id={"ep": dest}, device_id_type=MESH)

    def v_copy(dest):
        return pltpu.make_async_remote_copy(
            v_src(dest), v_buf.at[me], v_ss.at[dest], v_rs.at[me],
            device_id={"ep": dest}, device_id_type=MESH)

    for step in range(1, n):
        dest = lax.rem(me + step, n)
        if step % g == 0:
            k_copy(dest).start()
            v_copy(dest).start()
        q_copy(dest).start()

    def mate(step):
        return my_head * g + lax.rem(my_core + step, g)

    def recv(buf, sem, source):
        return pltpu.make_async_remote_copy(
            buf.at[source], buf.at[source], sem.at[source], sem.at[source],
            device_id={"ep": lax.rem(me + 1, n)}, device_id_type=MESH)

    def forward(source, step):
        to = mate(step)
        return (
            pltpu.make_async_remote_copy(
                k_buf.at[source], k_buf.at[source], fk_ss.at[source, step], fk_rs.at[source],
                device_id={"ep": to}, device_id_type=MESH),
            pltpu.make_async_remote_copy(
                v_buf.at[source], v_buf.at[source], fv_ss.at[source, step], fv_rs.at[source],
                device_id={"ep": to}, device_id_type=MESH),
        )

    for copy in own:
        copy.wait()

    lam = lam_ref[my_head]
    gain = gain_ref[...]
    key_row = lax.broadcasted_iota(jnp.int32, (rows, g_cols(sub)), 0)
    query_col = lax.broadcasted_iota(jnp.int32, (rows, g_cols(sub)), 1) % sub
    lane = lax.broadcasted_iota(jnp.int32, (sub, width), 1)

    def group(p, _):
        direct = p * g + my_core

        @pl.when(direct != me)
        def _():
            recv(k_buf, k_rs, direct).wait_recv()
            recv(v_buf, v_rs, direct).wait_recv()

        for step in range(1, g):
            for copy in forward(direct, step):
                copy.start()
        for step in range(1, g):
            other = p * g + lax.rem(my_core + step, g)
            recv(k_buf, fk_rs, other).wait_recv()
            recv(v_buf, fv_rs, other).wait_recv()

        def member(c, _):
            e = p * g + c
            vt_buf[e] = v_buf[e].astype(f32).T.astype(bf16)

            @pl.when(e != me)
            def _():
                recv(q_buf, q_rs, e).wait_recv()

            q = q_buf[e]
            zero = jnp.zeros_like(q)
            stacked = jnp.concatenate(
                [jnp.where(lane < width // 2, q, zero), jnp.where(lane < width // 2, zero, q)], axis=0)
            q_start = ((my_core + e) % g) * sub

            def scores_of(j):
                return lax.dot_general(
                    k_buf[j], stacked, (((1,), (1,)), ((), ())), preferred_element_type=f32)

            s = jnp.where(key_row <= query_col + q_start, scores_of(e), masked_low)
            m = jnp.max(s, axis=0, keepdims=True)
            weights = jnp.exp(s - m)
            l_buf[...] = jnp.sum(weights, axis=0, keepdims=True)
            m_buf[...] = m
            acc[...] = jnp.dot(vt_buf[e], weights.astype(bf16), preferred_element_type=f32)

            def block(j, _):
                s = scores_of(j)
                old = m_buf[...]
                m = jnp.maximum(old, jnp.max(s, axis=0, keepdims=True))
                weights = jnp.exp(s - m)
                scale = jnp.exp(old - m)
                l_buf[...] = l_buf[...] * scale + jnp.sum(weights, axis=0, keepdims=True)
                m_buf[...] = m
                acc[...] = acc[...] * scale + jnp.dot(
                    vt_buf[j], weights.astype(bf16), preferred_element_type=f32)
                return 0

            lax.fori_loop(0, e, block, 0)
            a = (acc[...] / l_buf[...]).T
            diff = a[:sub] - lam * a[sub:]
            inverse = lax.rsqrt(jnp.mean(diff * diff, axis=-1, keepdims=True) + norm_eps)
            hn_send[e] = (diff * inverse * gain).astype(bf16)

            @pl.when(e != me)
            def _():
                hn_copy(e).start()

            return 0

        lax.fori_loop(0, g, member, 0)
        return 0

    def hn_copy(dest):
        return pltpu.make_async_remote_copy(
            hn_send.at[dest], hn_buf.at[me], h_ss.at[dest], h_rs.at[me],
            device_id={"ep": dest}, device_id_type=MESH)

    lax.fori_loop(0, heads, group, 0)
    hn_buf[me] = hn_send[me]
    for step in range(1, n):
        source = lax.rem(me + step, n)
        recv(hn_buf, h_rs, source).wait_recv()
    w_copy.wait()
    for part in range(g):
        normed = jnp.concatenate(
            [hn_buf[h * g + lax.rem(part + me, g)] for h in range(heads)], axis=1)
        out_ref[part * sub : (part + 1) * sub, :] = jnp.dot(
            normed, w_buf[...], preferred_element_type=f32).astype(bf16)
    for step in range(1, n):
        dest = lax.rem(me + step, n)
        if step % g == 0:
            k_copy(dest).wait_send()
            v_copy(dest).wait_send()
        q_copy(dest).wait_send()
        hn_copy(dest).wait_send()
    for p in range(heads):
        for step in range(1, g):
            for copy in forward(p * g + my_core, step):
                copy.wait_send()


def g_cols(sub):
    return 2 * sub


def exchange_attention(query_pairs, key_pairs, value_rows, head_lambda, head_gain, out_weight):
    n = lax.axis_size("ep")
    rows = query_pairs.shape[0]
    heads = head_lambda.shape[0]
    width = query_pairs.shape[1] // heads
    head_size = width // 2
    vw = value_rows.shape[1] // heads
    sub = rows * heads // n
    positions = lax.axis_index("ep") * rows + jnp.arange(rows, dtype=jnp.int32)
    half = head_size // 2
    frequency = theta_base ** (-(jnp.arange(half, dtype=f32) * 2.0) / head_size)
    angles = positions.astype(f32)[:, None] * frequency[None, :]
    cosine, sine = jnp.cos(angles), jnp.sin(angles)
    cosines = jnp.concatenate([cosine] * 4, axis=1)
    sines = jnp.concatenate([-sine, sine] * 2, axis=1)
    turned = jax.ShapeDtypeStruct((heads, rows, width), bf16)
    rq, rk = pl.pallas_call(
        functools.partial(rotate_kernel, head_size, head_size ** (-0.5)),
        out_shape=(turned, turned),
        name="rotate",
    )(query_pairs, key_pairs, cosines, sines)
    any_spec = pl.BlockSpec(memory_space=pl.ANY)
    vmem = pl.BlockSpec(memory_space=pltpu.VMEM)
    dma = pltpu.SemaphoreType.DMA
    g = n // heads
    terms = pl.pallas_call(
        functools.partial(attention_kernel, n, heads),
        out_shape=jax.ShapeDtypeStruct((rows, out_weight.shape[1]), bf16),
        in_specs=[pl.BlockSpec(memory_space=pltpu.SMEM), vmem, any_spec, any_spec, any_spec, any_spec],
        out_specs=vmem,
        scratch_shapes=[
            pltpu.VMEM((n, sub, width), bf16),
            pltpu.VMEM((n, rows, width), bf16),
            pltpu.VMEM((n, rows, vw), bf16),
            pltpu.VMEM((n, vw, rows), bf16),
            pltpu.VMEM((n, sub, vw), bf16),
            pltpu.VMEM((n, sub, vw), bf16),
            pltpu.VMEM(out_weight.shape, bf16),
            pltpu.VMEM((vw, 2 * sub), f32),
            pltpu.VMEM((1, 2 * sub), f32),
            pltpu.VMEM((1, 2 * sub), f32),
            dma((n,)), dma((n,)), dma((n,)), dma((n,)), dma((n,)), dma((n,)),
            dma((n, g)), dma((n,)), dma((n, g)), dma((n,)),
            dma((n,)), dma((n,)), dma((3,)), dma(()),
        ],
        compiler_params=pltpu.CompilerParams(
            collective_id=0, has_side_effects=True, vmem_limit_bytes=40 * 2**20),
        cost_estimate=pl.CostEstimate(flops=20 * 10**9, bytes_accessed=8 * 2**20, transcendentals=5 * 10**6),
        name="attention",
    )(head_lambda, head_gain.reshape(1, vw), rq, rk, value_rows, out_weight)
    return lax.psum_scatter(terms, "tp", scatter_dimension=1, tiled=True)


def local(
    query_pairs,
    key_pairs,
    value_rows,
    head_lambda,
    head_gain,
    out_weight,
    moe_input,
    ffn_gain,
    routes,
    route_weight,
    gate_weight,
    up_weight,
    down_weight,
    shared_gate,
    shared_up,
    shared_down,
):
    n = lax.axis_size("ep")
    heads = head_lambda.shape[0]
    rows = query_pairs.shape[0]
    fits = n % heads == 0 and n // heads > 1 and (rows * heads) % (n * 64) == 0
    attention = exchange_attention if fits else generic_attention
    attn_out = attention(query_pairs, key_pairs, value_rows, head_lambda, head_gain, out_weight)
    row_values = moe_input.astype(jnp.float32)
    inverse_norm = lax.rsqrt(jnp.mean(row_values * row_values, axis=-1, keepdims=True) + norm_eps)
    normed = (row_values * inverse_norm * ffn_gain).astype(jnp.bfloat16)
    tokens, model = normed.shape
    n_tp = lax.axis_size("tp")
    capacity = tokens * TOP_K * 5 // (4 * n)
    part = lax.dynamic_slice_in_dim(normed, lax.axis_index("tp") * (model // n_tp), model // n_tp, axis=1)
    gathered = lax.all_gather(part, ("ep", "tp"), axis=0, tiled=False)
    gathered = gathered.reshape(n, n_tp, tokens, model // n_tp)
    all_routes = lax.all_gather(routes, "ep", axis=0, tiled=False)
    hit = jnp.any(all_routes == lax.axis_index("ep"), axis=-1)
    lower = jnp.tril(jnp.ones((tokens, tokens), bf16))
    rank = jnp.dot(hit.astype(bf16), lower.T, preferred_element_type=f32).astype(jnp.int32) - 1
    select = (hit[:, None, :] & (rank[:, None, :] == jnp.arange(capacity, dtype=jnp.int32)[None, :, None])).astype(bf16)
    arrived = jnp.einsum("bst,bhtd->bshd", select, gathered, preferred_element_type=f32).astype(bf16)
    arrived = arrived.reshape(n * capacity, model)
    gate_part = jnp.dot(arrived, gate_weight[0], preferred_element_type=jnp.float32)
    up_part = jnp.dot(arrived, up_weight[0], preferred_element_type=jnp.float32)
    hidden = (jax.nn.silu(gate_part) * up_part).astype(jnp.bfloat16)
    expert_terms = jnp.dot(hidden, down_weight[0], preferred_element_type=jnp.float32)
    shared_gated = jnp.dot(normed, shared_gate, preferred_element_type=jnp.float32)
    shared_lifted = jnp.dot(normed, shared_up, preferred_element_type=jnp.float32)
    shared_hidden = (jax.nn.silu(shared_gated) * shared_lifted).astype(jnp.bfloat16)
    shared_terms = jnp.dot(shared_hidden, shared_down, preferred_element_type=jnp.float32)
    both = jnp.concatenate([expert_terms.astype(bf16), shared_terms.astype(bf16)], axis=0)
    sums = lax.psum_scatter(both, "tp", scatter_dimension=1, tiled=True)
    expert_sum, shared_sum = sums[: n * capacity], sums[n * capacity :].astype(f32)
    returned = lax.all_to_all(expert_sum, "ep", split_axis=0, concat_axis=0, tiled=True)
    onehot = (routes[:, :, None] == jnp.arange(n, dtype=jnp.int32)).astype(bf16)
    named = jnp.sum(onehot, axis=1)
    ranks = jnp.dot(lower, named, preferred_element_type=f32) - 1.0
    slots = jnp.sum(onehot.astype(f32) * (ranks[:, None, :] + jnp.arange(n, dtype=f32) * capacity), axis=-1)
    moe_out = shared_sum
    for k in range(TOP_K):
        place = (slots[:, k : k + 1].astype(jnp.int32) == jnp.arange(n * capacity, dtype=jnp.int32)).astype(bf16)
        picked = jnp.dot(place, returned, preferred_element_type=f32)
        moe_out = moe_out + route_weight[:, k : k + 1] * picked
    moe_out = moe_out.astype(bf16)
    return (attn_out, moe_out)


def solution(mesh):
    return jax.shard_map(
        local,
        mesh=mesh,
        in_specs=(
            P("ep", "tp"),
            P("ep", "tp"),
            P("ep", "tp"),
            P("tp"),
            P(),
            P("tp", None),
            P("ep", None),
            P(),
            P("ep", None),
            P("ep", None),
            P("ep", None, "tp"),
            P("ep", None, "tp"),
            P("ep", "tp", None),
            P(None, "tp"),
            P(None, "tp"),
            P("tp", None),
        ),
        out_specs=(P("ep", "tp"), P("ep", "tp")),
        check_vma=False,
    )
```

```python
import functools

import jax
import jax.numpy as jnp
from jax import lax
from jax.experimental import pallas as pl
from jax.experimental.pallas import tpu as pltpu
from jax.sharding import PartitionSpec as P

TOP_K = 2
KEY_BLOCK = 128


theta_base = 500000.0
norm_eps = 1e-06
masked_low = -1e30


def rotate(inputs, positions):
    half_size = inputs.shape[-1] // 2
    frequency = theta_base ** (-(jnp.arange(half_size, dtype=jnp.float32) * 2.0) / inputs.shape[-1])
    angles = positions.astype(jnp.float32)[:, None] * frequency[None, :]
    cosine = jnp.cos(angles)[:, None, None, :]
    sine_part = jnp.sin(angles)[:, None, None, :]
    front_half = inputs[..., :half_size]
    back_half = inputs[..., half_size:]
    return jnp.concatenate(
        [front_half * cosine - back_half * sine_part, back_half * cosine + front_half * sine_part],
        axis=-1,
    )


def generic_attention(query_pairs, key_pairs, value_rows, head_lambda, head_gain, out_weight):
    local_rows = query_pairs.shape[0]
    local_heads = head_lambda.shape[0]
    head_size = query_pairs.shape[1] // (2 * local_heads)
    value_size = value_rows.shape[1] // local_heads
    positions = lax.axis_index("ep") * local_rows + jnp.arange(local_rows, dtype=jnp.int32)
    rot_queries = rotate(
        query_pairs.astype(jnp.float32).reshape(local_rows, local_heads, 2, head_size), positions
    ).astype(jnp.bfloat16)
    rot_keys = rotate(
        key_pairs.astype(jnp.float32).reshape(local_rows, local_heads, 2, head_size), positions
    ).astype(jnp.bfloat16)
    rot_keys = rot_keys.reshape(local_rows, local_heads * 2 * head_size)
    zero_init = (
        jnp.full((local_heads, 2, local_rows), masked_low, jnp.float32),
        jnp.zeros((local_heads, 2, local_rows), jnp.float32),
        jnp.zeros((local_heads, 2, local_rows, value_size), jnp.float32),
    )
    piece_keys = lax.all_gather(rot_keys, "ep", axis=0, tiled=True)
    piece_values = lax.all_gather(value_rows, "ep", axis=0, tiled=True)
    block_count = piece_keys.shape[0] // KEY_BLOCK
    group_size = 4
    group_count = block_count // group_size
    grouped_keys = piece_keys.reshape(group_count, group_size, KEY_BLOCK, local_heads, 2, head_size)
    grouped_values = piece_values.reshape(
        group_count, group_size, KEY_BLOCK, local_heads, value_size
    )

    def one_group(current, inputs):
        block_keys, block_values, group_index = inputs
        key_positions = group_index * group_size * KEY_BLOCK + jnp.arange(
            group_size * KEY_BLOCK, dtype=jnp.int32
        ).reshape(group_size, KEY_BLOCK)
        scores = jnp.einsum(
            "qhmd,gkhmd->hmqgk", rot_queries, block_keys, preferred_element_type=jnp.float32
        ) * head_size ** (-0.5)
        allowed = key_positions[None, :, :] <= positions[:, None, None]
        scores = jnp.where(allowed, scores, masked_low)
        block_max = jnp.max(scores, axis=-1)
        weights = jnp.where(allowed, jnp.exp(scores - block_max[..., None]), 0.0)
        block_sum = jnp.sum(weights, axis=-1)
        block_out = jnp.einsum(
            "hmqgk,gkhc->hmqgc",
            weights.astype(jnp.bfloat16),
            block_values,
            preferred_element_type=jnp.float32,
        )
        run_max, run_sum, run_out = current
        new_max = jnp.maximum(run_max, jnp.max(block_max, axis=-1))
        old_scale = jnp.exp(run_max - new_max)
        new_scale = jnp.exp(block_max - new_max[..., None])
        run_sum = run_sum * old_scale + jnp.sum(new_scale * block_sum, axis=-1)
        run_out = run_out * old_scale[..., None] + jnp.sum(
            new_scale[..., None] * block_out, axis=-2
        )
        return ((new_max, run_sum, run_out), None)

    result, _ = lax.scan(
        one_group,
        zero_init,
        (grouped_keys, grouped_values, jnp.arange(group_count, dtype=jnp.int32)),
    )
    run_max, run_sum, run_out = result
    map_outputs = run_out / run_sum[..., None]
    difference = map_outputs[:, 0] - head_lambda[:, None, None] * map_outputs[:, 1]
    inverse_rms = lax.rsqrt(jnp.mean(difference * difference, axis=-1, keepdims=True) + norm_eps)
    normed_heads = (difference * inverse_rms * head_gain).astype(jnp.bfloat16)
    head_rows = normed_heads.transpose(1, 0, 2).reshape(local_rows, local_heads * value_size)
    mixer_terms = jnp.dot(head_rows, out_weight, preferred_element_type=jnp.float32)
    attn_out = lax.psum_scatter(
        mixer_terms.astype(jnp.bfloat16), "tp", scatter_dimension=1, tiled=True
    )
    return attn_out


MESH = pl.DeviceIdType.MESH
f32, bf16 = jnp.float32, jnp.bfloat16


def rotate_kernel(head_size, scale, q_ref, k_ref, cos_ref, sin_ref, rq_ref, rk_ref):
    heads, _, width = rq_ref.shape
    half = head_size // 2
    lane = lax.broadcasted_iota(jnp.int32, (q_ref.shape[0], width), 1)
    front = lane % head_size < half
    cosine, sine = cos_ref[...], sin_ref[...]
    for source, target, factor in ((q_ref, rq_ref, scale), (k_ref, rk_ref, 1.0)):
        for h in range(heads):
            x = source[:, h * width : (h + 1) * width].astype(f32)
            partner = jnp.where(front, pltpu.roll(x, width - half, 1), pltpu.roll(x, half, 1))
            turned = (x * cosine + partner * sine).astype(bf16)
            target[h] = turned if factor == 1.0 else turned * jnp.asarray(factor, bf16)


def attention_kernel(
    n, heads, lam_ref, gain_ref, rq_ref, rk_ref, v_ref, w_ref, tok_ref, out_ref, arr_ref,
    q_buf, k_buf, v_buf, vt_buf, hn_send, hn_buf, w_buf, acc, m_buf, l_buf,
    q_ss, q_rs, k_ss, k_rs, v_ss, v_rs, fk_ss, fk_rs, fv_ss, fv_rs, h_ss, h_rs, loc, w_sem, t_ss, t_rs, x_ss, x_rs,
):
    me = lax.axis_index("ep")
    my_tp = lax.axis_index("tp")
    n_tp = arr_ref.shape[0]
    g = n // heads
    my_head, my_core = me // g, me % g
    rows = rk_ref.shape[1]
    sub = rows // g
    width = rk_ref.shape[2]
    vw = v_buf.shape[2]

    barrier = pltpu.get_barrier_semaphore()
    for step in range(1, n):
        pl.semaphore_signal(barrier, inc=1, device_id={"ep": lax.rem(me + step, n)}, device_id_type=MESH)
    for step in range(1, n_tp):
        pl.semaphore_signal(barrier, inc=1, device_id={"tp": lax.rem(my_tp + step, n_tp)}, device_id_type=MESH)
    w_copy = pltpu.make_async_copy(w_ref, w_buf, w_sem)
    w_copy.start()

    def q_src(dest):
        start = pl.multiple_of(((dest % g + me) % g) * sub, sub)
        return rq_ref.at[dest // g, pl.ds(start, sub), :]

    def v_src(dest):
        return v_ref.at[:, pl.ds(pl.multiple_of((dest // g) * vw, vw), vw)]

    own = (
        pltpu.make_async_copy(q_src(me), q_buf.at[me], loc.at[0]),
        pltpu.make_async_copy(rk_ref.at[my_head], k_buf.at[me], loc.at[1]),
        pltpu.make_async_copy(v_src(me), v_buf.at[me], loc.at[2]),
        pltpu.make_async_copy(tok_ref.at[me], arr_ref.at[my_tp, me], loc.at[3]),
    )
    for copy in own:
        copy.start()
    pl.semaphore_wait(barrier, n - 1 + n_tp - 1)

    def q_copy(dest):
        return pltpu.make_async_remote_copy(
            q_src(dest), q_buf.at[me], q_ss.at[dest], q_rs.at[me],
            device_id={"ep": dest}, device_id_type=MESH)

    def k_copy(dest):
        return pltpu.make_async_remote_copy(
            rk_ref.at[dest // g], k_buf.at[me], k_ss.at[dest], k_rs.at[me],
            device_id={"ep": dest}, device_id_type=MESH)

    def v_copy(dest):
        return pltpu.make_async_remote_copy(
            v_src(dest), v_buf.at[me], v_ss.at[dest], v_rs.at[me],
            device_id={"ep": dest}, device_id_type=MESH)

    def tok_copy(dest):
        return pltpu.make_async_remote_copy(
            tok_ref.at[dest], arr_ref.at[my_tp, me], t_ss.at[dest], t_rs.at[me],
            device_id={"ep": dest}, device_id_type=MESH)

    def tok_arrival(source):
        return pltpu.make_async_remote_copy(
            tok_ref.at[0], arr_ref.at[my_tp, source], t_ss.at[0], t_rs.at[source],
            device_id={"ep": lax.rem(me + 1, n)}, device_id_type=MESH)

    def tok_spread(dest):
        return pltpu.make_async_remote_copy(
            arr_ref.at[my_tp], arr_ref.at[my_tp], x_ss.at[dest], x_rs.at[my_tp],
            device_id={"tp": dest}, device_id_type=MESH)

    def spread_arrival(source):
        return pltpu.make_async_remote_copy(
            arr_ref.at[source], arr_ref.at[source], x_ss.at[source], x_rs.at[source],
            device_id={"tp": lax.rem(my_tp + 1, n_tp)}, device_id_type=MESH)

    for step in range(1, n):
        tok_copy(lax.rem(me + step, n)).start()
    for step in range(1, n):
        dest = lax.rem(me + step, n)
        if step % g == 0:
            k_copy(dest).start()
            v_copy(dest).start()
        q_copy(dest).start()

    def mate(step):
        return my_head * g + lax.rem(my_core + step, g)

    def recv(buf, sem, source):
        return pltpu.make_async_remote_copy(
            buf.at[source], buf.at[source], sem.at[source], sem.at[source],
            device_id={"ep": lax.rem(me + 1, n)}, device_id_type=MESH)

    def forward(source, step):
        to = mate(step)
        return (
            pltpu.make_async_remote_copy(
                k_buf.at[source], k_buf.at[source], fk_ss.at[source, step], fk_rs.at[source],
                device_id={"ep": to}, device_id_type=MESH),
            pltpu.make_async_remote_copy(
                v_buf.at[source], v_buf.at[source], fv_ss.at[source, step], fv_rs.at[source],
                device_id={"ep": to}, device_id_type=MESH),
        )

    for copy in own:
        copy.wait()

    lam = lam_ref[my_head]
    gain = gain_ref[...]
    key_row = lax.broadcasted_iota(jnp.int32, (rows, g_cols(sub)), 0)
    query_col = lax.broadcasted_iota(jnp.int32, (rows, g_cols(sub)), 1) % sub
    lane = lax.broadcasted_iota(jnp.int32, (sub, width), 1)

    def group(p, _):
        direct = p * g + my_core

        @pl.when(direct != me)
        def _():
            recv(k_buf, k_rs, direct).wait_recv()
            recv(v_buf, v_rs, direct).wait_recv()

        for step in range(1, g):
            for copy in forward(direct, step):
                copy.start()
        for step in range(1, g):
            other = p * g + lax.rem(my_core + step, g)
            recv(k_buf, fk_rs, other).wait_recv()
            recv(v_buf, fv_rs, other).wait_recv()

        def member(c, _):
            e = p * g + c
            vt_buf[e] = v_buf[e].astype(f32).T.astype(bf16)

            @pl.when(e != me)
            def _():
                recv(q_buf, q_rs, e).wait_recv()

            q = q_buf[e]
            zero = jnp.zeros_like(q)
            stacked = jnp.concatenate(
                [jnp.where(lane < width // 2, q, zero), jnp.where(lane < width // 2, zero, q)], axis=0)
            q_start = ((my_core + e) % g) * sub

            def scores_of(j):
                return lax.dot_general(
                    k_buf[j], stacked, (((1,), (1,)), ((), ())), preferred_element_type=f32)

            s = jnp.where(key_row <= query_col + q_start, scores_of(e), masked_low)
            m = jnp.max(s, axis=0, keepdims=True)
            weights = jnp.exp(s - m)
            l_buf[...] = jnp.sum(weights, axis=0, keepdims=True)
            m_buf[...] = m
            acc[...] = jnp.dot(vt_buf[e], weights.astype(bf16), preferred_element_type=f32)

            def block(j, _):
                s = scores_of(j)
                old = m_buf[...]
                m = jnp.maximum(old, jnp.max(s, axis=0, keepdims=True))
                weights = jnp.exp(s - m)
                scale = jnp.exp(old - m)
                l_buf[...] = l_buf[...] * scale + jnp.sum(weights, axis=0, keepdims=True)
                m_buf[...] = m
                acc[...] = acc[...] * scale + jnp.dot(
                    vt_buf[j], weights.astype(bf16), preferred_element_type=f32)
                return 0

            lax.fori_loop(0, e, block, 0)
            a = (acc[...] / l_buf[...]).T
            diff = a[:sub] - lam * a[sub:]
            inverse = lax.rsqrt(jnp.mean(diff * diff, axis=-1, keepdims=True) + norm_eps)
            hn_send[e] = (diff * inverse * gain).astype(bf16)

            @pl.when(e != me)
            def _():
                hn_copy(e).start()

            return 0

        lax.fori_loop(0, g, member, 0)

        @pl.when(p == 0)
        def _():
            for step in range(1, n):
                tok_arrival(lax.rem(me + step, n)).wait_recv()
            for step in range(1, n_tp):
                tok_spread(lax.rem(my_tp + step, n_tp)).start()

        return 0

    def hn_copy(dest):
        return pltpu.make_async_remote_copy(
            hn_send.at[dest], hn_buf.at[me], h_ss.at[dest], h_rs.at[me],
            device_id={"ep": dest}, device_id_type=MESH)

    lax.fori_loop(0, heads, group, 0)
    hn_buf[me] = hn_send[me]
    for step in range(1, n):
        source = lax.rem(me + step, n)
        recv(hn_buf, h_rs, source).wait_recv()
    w_copy.wait()
    for part in range(g):
        normed = jnp.concatenate(
            [hn_buf[h * g + lax.rem(part + me, g)] for h in range(heads)], axis=1)
        for t in range(n_tp):
            piece = out_ref.shape[2]
            out_ref[t, part * sub : (part + 1) * sub, :] = jnp.dot(
                normed, w_buf[:, t * piece : (t + 1) * piece], preferred_element_type=f32).astype(bf16)
    for step in range(1, n):
        dest = lax.rem(me + step, n)
        if step % g == 0:
            k_copy(dest).wait_send()
            v_copy(dest).wait_send()
        q_copy(dest).wait_send()
        hn_copy(dest).wait_send()
        tok_copy(dest).wait_send()
    for step in range(1, n_tp):
        other = lax.rem(my_tp + step, n_tp)
        spread_arrival(other).wait_recv()
        tok_spread(other).wait_send()
    for p in range(heads):
        for step in range(1, g):
            for copy in forward(p * g + my_core, step):
                copy.wait_send()


def g_cols(sub):
    return 2 * sub


def exchange_attention(query_pairs, key_pairs, value_rows, head_lambda, head_gain, out_weight, outgoing):
    n = lax.axis_size("ep")
    rows = query_pairs.shape[0]
    heads = head_lambda.shape[0]
    width = query_pairs.shape[1] // heads
    head_size = width // 2
    vw = value_rows.shape[1] // heads
    sub = rows * heads // n
    positions = lax.axis_index("ep") * rows + jnp.arange(rows, dtype=jnp.int32)
    half = head_size // 2
    frequency = theta_base ** (-(jnp.arange(half, dtype=f32) * 2.0) / head_size)
    angles = positions.astype(f32)[:, None] * frequency[None, :]
    cosine, sine = jnp.cos(angles), jnp.sin(angles)
    cosines = jnp.concatenate([cosine] * 4, axis=1)
    sines = jnp.concatenate([-sine, sine] * 2, axis=1)
    turned = jax.ShapeDtypeStruct((heads, rows, width), bf16)
    rq, rk = pl.pallas_call(
        functools.partial(rotate_kernel, head_size, head_size ** (-0.5)),
        out_shape=(turned, turned),
        name="rotate",
    )(query_pairs, key_pairs, cosines, sines)
    any_spec = pl.BlockSpec(memory_space=pl.ANY)
    vmem = pl.BlockSpec(memory_space=pltpu.VMEM)
    dma = pltpu.SemaphoreType.DMA
    g = n // heads
    n_tp = lax.axis_size("tp")
    return pl.pallas_call(
        functools.partial(attention_kernel, n, heads),
        out_shape=(
            jax.ShapeDtypeStruct((n_tp, rows, out_weight.shape[1] // n_tp), bf16),
            jax.ShapeDtypeStruct((n_tp,) + outgoing.shape, bf16),
        ),
        in_specs=[pl.BlockSpec(memory_space=pltpu.SMEM), vmem] + [any_spec] * 5,
        out_specs=(vmem, any_spec),
        scratch_shapes=[
            pltpu.VMEM((n, sub, width), bf16),
            pltpu.VMEM((n, rows, width), bf16),
            pltpu.VMEM((n, rows, vw), bf16),
            pltpu.VMEM((n, vw, rows), bf16),
            pltpu.VMEM((n, sub, vw), bf16),
            pltpu.VMEM((n, sub, vw), bf16),
            pltpu.VMEM(out_weight.shape, bf16),
            pltpu.VMEM((vw, 2 * sub), f32),
            pltpu.VMEM((1, 2 * sub), f32),
            pltpu.VMEM((1, 2 * sub), f32),
            dma((n,)), dma((n,)), dma((n,)), dma((n,)), dma((n,)), dma((n,)),
            dma((n, g)), dma((n,)), dma((n, g)), dma((n,)),
            dma((n,)), dma((n,)), dma((4,)), dma(()),
            dma((n,)), dma((n,)), dma((n_tp,)), dma((n_tp,)),
        ],
        compiler_params=pltpu.CompilerParams(
            collective_id=0, has_side_effects=True, vmem_limit_bytes=40 * 2**20),
        cost_estimate=pl.CostEstimate(flops=20 * 10**9, bytes_accessed=8 * 2**20, transcendentals=5 * 10**6),
        name="attention",
    )(head_lambda, head_gain.reshape(1, vw), rq, rk, value_rows, out_weight, outgoing)


def expert_kernel(
    n, n_tp, mix_ref, arr_ref, xn_ref, place_ref, rw_ref, wg_ref, wu_ref, wd_ref, sg_ref, su_ref, sd_ref,
    attn_ref, moe_ref,
    mix_in, arr, wg, wu, wd, sg, su, sd, sh_send, sh_in, ex_send, ex_in, y_buf, ret,
    loc, m_ss, m_rs, s_ss, s_rs, e_ss, e_rs, y_ss, y_rs,
):
    me = lax.axis_index("ep")
    my_tp = lax.axis_index("tp")
    piece = moe_ref.shape[1]
    cap = y_buf.shape[1]
    barrier = pltpu.get_barrier_semaphore()
    for step in range(1, n):
        pl.semaphore_signal(barrier, inc=1, device_id={"ep": lax.rem(me + step, n)}, device_id_type=MESH)
    for step in range(1, n_tp):
        pl.semaphore_signal(barrier, inc=1, device_id={"tp": lax.rem(my_tp + step, n_tp)}, device_id_type=MESH)
    loads = [
        pltpu.make_async_copy(source, target, loc.at[i])
        for i, (source, target) in enumerate((
            (sg_ref, sg), (su_ref, su), (sd_ref, sd), (arr_ref, arr),
            (wg_ref.at[0], wg), (wu_ref.at[0], wu), (wd_ref.at[0], wd),
            (mix_ref.at[my_tp], mix_in.at[my_tp])))
    ]
    for load in loads:
        load.start()
    pl.semaphore_wait(barrier, n - 1 + n_tp - 1)

    def scatter(send, into, send_sems, recv_sems, dest):
        return pltpu.make_async_remote_copy(
            send.at[dest], into.at[my_tp], send_sems.at[dest], recv_sems.at[my_tp],
            device_id={"tp": dest}, device_id_type=MESH)

    def arrival(into, recv_sems, source, axis):
        return pltpu.make_async_remote_copy(
            into.at[source], into.at[source], recv_sems.at[source], recv_sems.at[source],
            device_id={axis: lax.rem(lax.axis_index(axis) + 1, n if axis == "ep" else n_tp)},
            device_id_type=MESH)

    peers = [lax.rem(my_tp + step, n_tp) for step in (*range(1, n_tp), 0)]
    for dest in peers[:-1]:
        scatter(mix_ref, mix_in, m_ss, m_rs, dest).start()

    def columns(dest):
        return pl.ds(pl.multiple_of(dest * piece, piece), piece)

    def gated(gate, up):
        return (gate / (1.0 + jnp.exp(-gate)) * up).astype(bf16)

    for i in (0, 1, 2):
        loads[i].wait()
    xn = xn_ref[...]
    hidden = gated(
        jnp.dot(xn, sg[...], preferred_element_type=f32),
        jnp.dot(xn, su[...], preferred_element_type=f32))
    for dest in peers:
        sh_send[dest] = jnp.dot(hidden, sd[:, columns(dest)], preferred_element_type=f32).astype(bf16)
    for i in (3, 4, 5, 6):
        loads[i].wait()
    gate = up = None
    for t in range(n_tp):
        rows = arr[t].reshape(n * cap, piece)
        span = slice(t * piece, (t + 1) * piece)
        gate_part = jnp.dot(rows, wg[span, :], preferred_element_type=f32)
        up_part = jnp.dot(rows, wu[span, :], preferred_element_type=f32)
        gate = gate_part if gate is None else gate + gate_part
        up = up_part if up is None else up + up_part
    hidden = gated(gate, up)
    for dest in peers:
        ex_send[dest] = jnp.dot(hidden, wd[:, columns(dest)], preferred_element_type=f32).astype(bf16)
        if dest is not peers[-1]:
            scatter(ex_send, ex_in, e_ss, e_rs, dest).start()
    for dest in peers[:-1]:
        scatter(sh_send, sh_in, s_ss, s_rs, dest).start()
    loads[7].wait()
    for source in peers[:-1]:
        arrival(mix_in, m_rs, source, "tp").wait_recv()
    total = mix_in[0].astype(f32)
    for t in range(1, n_tp):
        total = total + mix_in[t].astype(f32)
    attn_ref[...] = total.astype(bf16)

    def y_copy(dest):
        return pltpu.make_async_remote_copy(
            y_buf.at[dest], ret.at[me], y_ss.at[dest], y_rs.at[me],
            device_id={"ep": dest}, device_id_type=MESH)

    y = ex_send[my_tp].astype(f32)
    for source in peers[:-1]:
        arrival(ex_in, e_rs, source, "tp").wait_recv()
        y = y + ex_in[source].astype(f32)
    y_buf[...] = y.astype(bf16).reshape(n, cap, piece)
    for step in range(1, n):
        y_copy(lax.rem(me + step, n)).start()
    ret[me] = y_buf[me]
    out = sh_send[my_tp].astype(f32)
    for source in peers[:-1]:
        arrival(sh_in, s_rs, source, "tp").wait_recv()
        out = out + sh_in[source].astype(f32)
    for step in range(1, n):
        arrival(ret, y_rs, lax.rem(me + step, n), "ep").wait_recv()
    returned = ret[...].reshape(n * cap, piece)
    for k in range(place_ref.shape[0]):
        out = out + rw_ref[:, k : k + 1] * jnp.dot(place_ref[k], returned, preferred_element_type=f32)
    moe_ref[...] = out.astype(bf16)
    for dest in peers[:-1]:
        scatter(mix_ref, mix_in, m_ss, m_rs, dest).wait_send()
        scatter(ex_send, ex_in, e_ss, e_rs, dest).wait_send()
        scatter(sh_send, sh_in, s_ss, s_rs, dest).wait_send()
    for step in range(1, n):
        y_copy(lax.rem(me + step, n)).wait_send()


def exchange_all(
    query_pairs, key_pairs, value_rows, head_lambda, head_gain, out_weight, normed, routes, route_weight,
    gate_weight, up_weight, down_weight, shared_gate, shared_up, shared_down,
):
    n, n_tp = lax.axis_size("ep"), lax.axis_size("tp")
    tokens, model = normed.shape
    piece = model // n_tp
    rows = query_pairs.shape[0]
    cap = -(-(tokens * TOP_K * 5 // (4 * n)) // 16) * 16
    onehot = (routes[:, :, None] == jnp.arange(n, dtype=jnp.int32)).astype(bf16)
    lower = jnp.tril(jnp.ones((tokens, tokens), bf16))
    ranks = jnp.dot(lower, jnp.sum(onehot, axis=1), preferred_element_type=f32) - 1.0
    slots = jnp.sum(onehot.astype(f32) * (ranks[:, None, :] + jnp.arange(n, dtype=f32) * cap), axis=-1)
    slots = slots.astype(jnp.int32).T
    place = (slots[:, :, None] == jnp.arange(n * cap, dtype=jnp.int32)).astype(bf16)
    part = lax.dynamic_slice_in_dim(normed, lax.axis_index("tp") * piece, piece, axis=1)
    outgoing = lax.dot_general(
        jnp.sum(place, axis=0), part, (((0,), (0,)), ((), ())), preferred_element_type=f32).astype(bf16)
    mix, arr = exchange_attention(
        query_pairs, key_pairs, value_rows, head_lambda, head_gain, out_weight, outgoing.reshape(n, cap, piece))
    any_spec = pl.BlockSpec(memory_space=pl.ANY)
    vmem = pl.BlockSpec(memory_space=pltpu.VMEM)
    dma = pltpu.SemaphoreType.DMA
    hidden, shared = gate_weight.shape[2], shared_gate.shape[1]
    return pl.pallas_call(
        functools.partial(expert_kernel, n, n_tp),
        out_shape=(
            jax.ShapeDtypeStruct((rows, piece), bf16),
            jax.ShapeDtypeStruct((tokens, piece), bf16),
        ),
        in_specs=[any_spec, any_spec, vmem, vmem, vmem] + [any_spec] * 6,
        out_specs=(vmem, vmem),
        scratch_shapes=[
            pltpu.VMEM((n_tp, rows, piece), bf16),
            pltpu.VMEM((n_tp, n, cap, piece), bf16),
            pltpu.VMEM((model, hidden), bf16),
            pltpu.VMEM((model, hidden), bf16),
            pltpu.VMEM((hidden, model), bf16),
            pltpu.VMEM((model, shared), bf16),
            pltpu.VMEM((model, shared), bf16),
            pltpu.VMEM((shared, model), bf16),
            pltpu.VMEM((n_tp, tokens, piece), bf16),
            pltpu.VMEM((n_tp, tokens, piece), bf16),
            pltpu.VMEM((n_tp, n * cap, piece), bf16),
            pltpu.VMEM((n_tp, n * cap, piece), bf16),
            pltpu.VMEM((n, cap, piece), bf16),
            pltpu.VMEM((n, cap, piece), bf16),
            dma((8,)), dma((n_tp,)), dma((n_tp,)), dma((n_tp,)), dma((n_tp,)), dma((n_tp,)), dma((n_tp,)),
            dma((n,)), dma((n,)),
        ],
        compiler_params=pltpu.CompilerParams(
            collective_id=1, has_side_effects=True, vmem_limit_bytes=48 * 2**20),
        cost_estimate=pl.CostEstimate(flops=10 * 10**9, bytes_accessed=16 * 2**20, transcendentals=5 * 10**5),
        name="experts",
    )(mix, arr, normed, place, route_weight, gate_weight, up_weight, down_weight, shared_gate, shared_up, shared_down)


def local(
    query_pairs,
    key_pairs,
    value_rows,
    head_lambda,
    head_gain,
    out_weight,
    moe_input,
    ffn_gain,
    routes,
    route_weight,
    gate_weight,
    up_weight,
    down_weight,
    shared_gate,
    shared_up,
    shared_down,
):
    n = lax.axis_size("ep")
    heads = head_lambda.shape[0]
    rows = query_pairs.shape[0]
    fits = n % heads == 0 and n // heads > 1 and (rows * heads) % (n * 64) == 0
    row_values = moe_input.astype(jnp.float32)
    inverse_norm = lax.rsqrt(jnp.mean(row_values * row_values, axis=-1, keepdims=True) + norm_eps)
    normed = (row_values * inverse_norm * ffn_gain).astype(jnp.bfloat16)
    if fits:
        return exchange_all(
            query_pairs, key_pairs, value_rows, head_lambda, head_gain, out_weight, normed, routes, route_weight,
            gate_weight, up_weight, down_weight, shared_gate, shared_up, shared_down,
        )
    attn_out = generic_attention(query_pairs, key_pairs, value_rows, head_lambda, head_gain, out_weight)
    token_rows = normed.shape[0]
    experts = lax.axis_size("ep")
    capacity = token_rows * TOP_K * 5 // (4 * experts)
    flat_routes = routes.reshape(-1)
    onehot = (flat_routes[:, None] == jnp.arange(experts, dtype=jnp.int32)).astype(jnp.int32)
    slot_rank = jnp.sum((jnp.cumsum(onehot, axis=0) - 1) * onehot, axis=-1)
    slot_index = flat_routes * capacity + slot_rank
    token_index = jnp.arange(token_rows * TOP_K, dtype=jnp.int32) // TOP_K
    slot_rows = (
        jnp.full((experts * capacity,), token_rows, jnp.int32).at[slot_index].set(token_index)
    )
    padded = jnp.concatenate([normed, jnp.zeros((1, normed.shape[1]), jnp.bfloat16)], axis=0)
    outgoing = padded[slot_rows]
    arrived = lax.all_to_all(outgoing, "ep", split_axis=0, concat_axis=0, tiled=True)
    gate_part = jnp.dot(arrived, gate_weight[0], preferred_element_type=jnp.float32)
    up_part = jnp.dot(arrived, up_weight[0], preferred_element_type=jnp.float32)
    hidden = (jax.nn.silu(gate_part) * up_part).astype(jnp.bfloat16)
    expert_terms = jnp.dot(hidden, down_weight[0], preferred_element_type=jnp.float32)
    shared_gated = jnp.dot(normed, shared_gate, preferred_element_type=jnp.float32)
    shared_lifted = jnp.dot(normed, shared_up, preferred_element_type=jnp.float32)
    shared_hidden = (jax.nn.silu(shared_gated) * shared_lifted).astype(jnp.bfloat16)
    shared_terms = jnp.dot(shared_hidden, shared_down, preferred_element_type=jnp.float32)
    expert_sum, shared_sum = (
        lax.psum_scatter(
            expert_terms.astype(jnp.bfloat16), "tp", scatter_dimension=1, tiled=True
        ).astype(jnp.float32),
        lax.psum_scatter(
            shared_terms.astype(jnp.bfloat16), "tp", scatter_dimension=1, tiled=True
        ).astype(jnp.float32),
    )
    returned = lax.all_to_all(
        expert_sum.astype(jnp.bfloat16), "ep", split_axis=0, concat_axis=0, tiled=True
    )
    picked = returned[slot_index.reshape(token_rows, TOP_K)]
    moe_out = (
        jnp.sum(route_weight[..., None] * picked.astype(jnp.float32), axis=1) + shared_sum
    ).astype(jnp.bfloat16)
    return (attn_out, moe_out)


def solution(mesh):
    return jax.shard_map(
        local,
        mesh=mesh,
        in_specs=(
            P("ep", "tp"),
            P("ep", "tp"),
            P("ep", "tp"),
            P("tp"),
            P(),
            P("tp", None),
            P("ep", None),
            P(),
            P("ep", None),
            P("ep", None),
            P("ep", None, "tp"),
            P("ep", None, "tp"),
            P("ep", "tp", None),
            P(None, "tp"),
            P(None, "tp"),
            P("tp", None),
        ),
        out_specs=(P("ep", "tp"), P("ep", "tp")),
        check_vma=False,
    )
```

```python
import functools

import jax
import jax.numpy as jnp
from jax import lax
from jax.experimental import pallas as pl
from jax.experimental.pallas import tpu as pltpu
from jax.sharding import PartitionSpec as P

TOP_K = 2
KEY_BLOCK = 128


theta_base = 500000.0
norm_eps = 1e-06
masked_low = -1e30


def rotate(inputs, positions):
    half_size = inputs.shape[-1] // 2
    frequency = theta_base ** (-(jnp.arange(half_size, dtype=jnp.float32) * 2.0) / inputs.shape[-1])
    angles = positions.astype(jnp.float32)[:, None] * frequency[None, :]
    cosine = jnp.cos(angles)[:, None, None, :]
    sine_part = jnp.sin(angles)[:, None, None, :]
    front_half = inputs[..., :half_size]
    back_half = inputs[..., half_size:]
    return jnp.concatenate(
        [front_half * cosine - back_half * sine_part, back_half * cosine + front_half * sine_part],
        axis=-1,
    )


def generic_attention(query_pairs, key_pairs, value_rows, head_lambda, head_gain, out_weight):
    local_rows = query_pairs.shape[0]
    local_heads = head_lambda.shape[0]
    head_size = query_pairs.shape[1] // (2 * local_heads)
    value_size = value_rows.shape[1] // local_heads
    positions = lax.axis_index("ep") * local_rows + jnp.arange(local_rows, dtype=jnp.int32)
    rot_queries = rotate(
        query_pairs.astype(jnp.float32).reshape(local_rows, local_heads, 2, head_size), positions
    ).astype(jnp.bfloat16)
    rot_keys = rotate(
        key_pairs.astype(jnp.float32).reshape(local_rows, local_heads, 2, head_size), positions
    ).astype(jnp.bfloat16)
    rot_keys = rot_keys.reshape(local_rows, local_heads * 2 * head_size)
    zero_init = (
        jnp.full((local_heads, 2, local_rows), masked_low, jnp.float32),
        jnp.zeros((local_heads, 2, local_rows), jnp.float32),
        jnp.zeros((local_heads, 2, local_rows, value_size), jnp.float32),
    )
    piece_keys = lax.all_gather(rot_keys, "ep", axis=0, tiled=True)
    piece_values = lax.all_gather(value_rows, "ep", axis=0, tiled=True)
    block_count = piece_keys.shape[0] // KEY_BLOCK
    group_size = 4
    group_count = block_count // group_size
    grouped_keys = piece_keys.reshape(group_count, group_size, KEY_BLOCK, local_heads, 2, head_size)
    grouped_values = piece_values.reshape(
        group_count, group_size, KEY_BLOCK, local_heads, value_size
    )

    def one_group(current, inputs):
        block_keys, block_values, group_index = inputs
        key_positions = group_index * group_size * KEY_BLOCK + jnp.arange(
            group_size * KEY_BLOCK, dtype=jnp.int32
        ).reshape(group_size, KEY_BLOCK)
        scores = jnp.einsum(
            "qhmd,gkhmd->hmqgk", rot_queries, block_keys, preferred_element_type=jnp.float32
        ) * head_size ** (-0.5)
        allowed = key_positions[None, :, :] <= positions[:, None, None]
        scores = jnp.where(allowed, scores, masked_low)
        block_max = jnp.max(scores, axis=-1)
        weights = jnp.where(allowed, jnp.exp(scores - block_max[..., None]), 0.0)
        block_sum = jnp.sum(weights, axis=-1)
        block_out = jnp.einsum(
            "hmqgk,gkhc->hmqgc",
            weights.astype(jnp.bfloat16),
            block_values,
            preferred_element_type=jnp.float32,
        )
        run_max, run_sum, run_out = current
        new_max = jnp.maximum(run_max, jnp.max(block_max, axis=-1))
        old_scale = jnp.exp(run_max - new_max)
        new_scale = jnp.exp(block_max - new_max[..., None])
        run_sum = run_sum * old_scale + jnp.sum(new_scale * block_sum, axis=-1)
        run_out = run_out * old_scale[..., None] + jnp.sum(
            new_scale[..., None] * block_out, axis=-2
        )
        return ((new_max, run_sum, run_out), None)

    result, _ = lax.scan(
        one_group,
        zero_init,
        (grouped_keys, grouped_values, jnp.arange(group_count, dtype=jnp.int32)),
    )
    run_max, run_sum, run_out = result
    map_outputs = run_out / run_sum[..., None]
    difference = map_outputs[:, 0] - head_lambda[:, None, None] * map_outputs[:, 1]
    inverse_rms = lax.rsqrt(jnp.mean(difference * difference, axis=-1, keepdims=True) + norm_eps)
    normed_heads = (difference * inverse_rms * head_gain).astype(jnp.bfloat16)
    head_rows = normed_heads.transpose(1, 0, 2).reshape(local_rows, local_heads * value_size)
    mixer_terms = jnp.dot(head_rows, out_weight, preferred_element_type=jnp.float32)
    attn_out = lax.psum_scatter(
        mixer_terms.astype(jnp.bfloat16), "tp", scatter_dimension=1, tiled=True
    )
    return attn_out


MESH = pl.DeviceIdType.MESH
f32, bf16 = jnp.float32, jnp.bfloat16


def rotate_kernel(head_size, scale, q_ref, k_ref, cos_ref, sin_ref, rq_ref, rk_ref):
    heads, _, width = rq_ref.shape
    half = head_size // 2
    lane = lax.broadcasted_iota(jnp.int32, (q_ref.shape[0], width), 1)
    front = lane % head_size < half
    cosine, sine = cos_ref[...], sin_ref[...]
    for source, target, factor in ((q_ref, rq_ref, scale), (k_ref, rk_ref, 1.0)):
        for h in range(heads):
            x = source[:, h * width : (h + 1) * width].astype(f32)
            partner = jnp.where(front, pltpu.roll(x, width - half, 1), pltpu.roll(x, half, 1))
            turned = (x * cosine + partner * sine).astype(bf16)
            target[h] = turned if factor == 1.0 else turned * jnp.asarray(factor, bf16)


def attention_kernel(
    n, heads, lam_ref, gain_ref, rq_ref, rk_ref, v_ref, w_ref, tok_ref, out_ref, arr_ref,
    q_buf, k_buf, v_buf, vt_buf, hn_send, hn_buf, w_buf, acc, m_buf, l_buf,
    q_ss, q_rs, k_ss, k_rs, v_ss, v_rs, fk_ss, fk_rs, fv_ss, fv_rs, h_ss, h_rs, loc, w_sem, t_ss, t_rs, x_ss, x_rs,
):
    me = lax.axis_index("ep")
    my_tp = lax.axis_index("tp")
    n_tp = arr_ref.shape[0]
    g = n // heads
    my_head, my_core = me // g, me % g
    rows = rk_ref.shape[1]
    sub = rows // g
    width = rk_ref.shape[2]
    vw = v_buf.shape[2]

    barrier = pltpu.get_barrier_semaphore()
    for step in range(1, n):
        pl.semaphore_signal(barrier, inc=1, device_id={"ep": lax.rem(me + step, n)}, device_id_type=MESH)
    for step in range(1, n_tp):
        pl.semaphore_signal(barrier, inc=1, device_id={"tp": lax.rem(my_tp + step, n_tp)}, device_id_type=MESH)
    w_copy = pltpu.make_async_copy(w_ref, w_buf, w_sem)
    w_copy.start()

    def q_src(dest):
        start = pl.multiple_of(((dest % g + me) % g) * sub, sub)
        return rq_ref.at[dest // g, pl.ds(start, sub), :]

    def v_src(dest):
        return v_ref.at[:, pl.ds(pl.multiple_of((dest // g) * vw, vw), vw)]

    own = (
        pltpu.make_async_copy(q_src(me), q_buf.at[me], loc.at[0]),
        pltpu.make_async_copy(rk_ref.at[my_head], k_buf.at[me], loc.at[1]),
        pltpu.make_async_copy(v_src(me), v_buf.at[me], loc.at[2]),
        pltpu.make_async_copy(tok_ref.at[me], arr_ref.at[my_tp, me], loc.at[3]),
    )
    for copy in own:
        copy.start()
    pl.semaphore_wait(barrier, n - 1 + n_tp - 1)

    def q_copy(dest):
        return pltpu.make_async_remote_copy(
            q_src(dest), q_buf.at[me], q_ss.at[dest], q_rs.at[me],
            device_id={"ep": dest}, device_id_type=MESH)

    def k_copy(dest):
        return pltpu.make_async_remote_copy(
            rk_ref.at[dest // g], k_buf.at[me], k_ss.at[dest], k_rs.at[me],
            device_id={"ep": dest}, device_id_type=MESH)

    def v_copy(dest):
        return pltpu.make_async_remote_copy(
            v_src(dest), v_buf.at[me], v_ss.at[dest], v_rs.at[me],
            device_id={"ep": dest}, device_id_type=MESH)

    def tok_copy(dest):
        return pltpu.make_async_remote_copy(
            tok_ref.at[dest], arr_ref.at[my_tp, me], t_ss.at[dest], t_rs.at[me],
            device_id={"ep": dest}, device_id_type=MESH)

    def tok_arrival(source):
        return pltpu.make_async_remote_copy(
            tok_ref.at[0], arr_ref.at[my_tp, source], t_ss.at[0], t_rs.at[source],
            device_id={"ep": lax.rem(me + 1, n)}, device_id_type=MESH)

    def tok_spread(dest):
        return pltpu.make_async_remote_copy(
            arr_ref.at[my_tp], arr_ref.at[my_tp], x_ss.at[dest], x_rs.at[my_tp],
            device_id={"tp": dest}, device_id_type=MESH)

    def spread_arrival(source):
        return pltpu.make_async_remote_copy(
            arr_ref.at[source], arr_ref.at[source], x_ss.at[source], x_rs.at[source],
            device_id={"tp": lax.rem(my_tp + 1, n_tp)}, device_id_type=MESH)

    for step in range(1, n):
        tok_copy(lax.rem(me + step, n)).start()
    for step in range(1, n):
        dest = lax.rem(me + step, n)
        if step % g == 0:
            k_copy(dest).start()
            v_copy(dest).start()
        q_copy(dest).start()

    def mate(step):
        return my_head * g + lax.rem(my_core + step, g)

    def recv(buf, sem, source):
        return pltpu.make_async_remote_copy(
            buf.at[source], buf.at[source], sem.at[source], sem.at[source],
            device_id={"ep": lax.rem(me + 1, n)}, device_id_type=MESH)

    def forward(source, step):
        to = mate(step)
        return (
            pltpu.make_async_remote_copy(
                k_buf.at[source], k_buf.at[source], fk_ss.at[source, step], fk_rs.at[source],
                device_id={"ep": to}, device_id_type=MESH),
            pltpu.make_async_remote_copy(
                v_buf.at[source], v_buf.at[source], fv_ss.at[source, step], fv_rs.at[source],
                device_id={"ep": to}, device_id_type=MESH),
        )

    for copy in own:
        copy.wait()

    lam = lam_ref[my_head]
    gain = gain_ref[...]
    key_row = lax.broadcasted_iota(jnp.int32, (rows, g_cols(sub)), 0)
    query_col = lax.broadcasted_iota(jnp.int32, (rows, g_cols(sub)), 1) % sub
    lane = lax.broadcasted_iota(jnp.int32, (sub, width), 1)

    def group(p, _):
        direct = p * g + my_core

        @pl.when(direct != me)
        def _():
            recv(k_buf, k_rs, direct).wait_recv()
            recv(v_buf, v_rs, direct).wait_recv()

        for step in range(1, g):
            for copy in forward(direct, step):
                copy.start()
        for step in range(1, g):
            other = p * g + lax.rem(my_core + step, g)
            recv(k_buf, fk_rs, other).wait_recv()
            recv(v_buf, fv_rs, other).wait_recv()

        def member(c, _):
            e = p * g + c
            vt_buf[e] = v_buf[e].astype(f32).T.astype(bf16)

            @pl.when(e != me)
            def _():
                recv(q_buf, q_rs, e).wait_recv()

            q = q_buf[e]
            zero = jnp.zeros_like(q)
            stacked = jnp.concatenate(
                [jnp.where(lane < width // 2, q, zero), jnp.where(lane < width // 2, zero, q)], axis=0)
            q_start = ((my_core + e) % g) * sub

            def scores_of(j):
                return lax.dot_general(
                    k_buf[j], stacked, (((1,), (1,)), ((), ())), preferred_element_type=f32)

            s = jnp.where(key_row <= query_col + q_start, scores_of(e), masked_low)
            m = jnp.max(s, axis=0, keepdims=True)
            weights = jnp.exp(s - m)
            l_buf[...] = jnp.sum(weights, axis=0, keepdims=True)
            m_buf[...] = m
            acc[...] = jnp.dot(vt_buf[e], weights.astype(bf16), preferred_element_type=f32)

            def block(j, _):
                s = scores_of(j)
                old = m_buf[...]
                m = jnp.maximum(old, jnp.max(s, axis=0, keepdims=True))
                weights = jnp.exp(s - m)
                scale = jnp.exp(old - m)
                l_buf[...] = l_buf[...] * scale + jnp.sum(weights, axis=0, keepdims=True)
                m_buf[...] = m
                acc[...] = acc[...] * scale + jnp.dot(
                    vt_buf[j], weights.astype(bf16), preferred_element_type=f32)
                return 0

            lax.fori_loop(0, e, block, 0)
            a = (acc[...] / l_buf[...]).T
            diff = a[:sub] - lam * a[sub:]
            inverse = lax.rsqrt(jnp.mean(diff * diff, axis=-1, keepdims=True) + norm_eps)
            hn_send[e] = (diff * inverse * gain).astype(bf16)

            @pl.when(e != me)
            def _():
                hn_copy(e).start()

            return 0

        lax.fori_loop(0, g, member, 0)

        @pl.when(p == 0)
        def _():
            for step in range(1, n):
                tok_arrival(lax.rem(me + step, n)).wait_recv()
            for step in range(1, n_tp):
                tok_spread(lax.rem(my_tp + step, n_tp)).start()

        return 0

    def hn_copy(dest):
        return pltpu.make_async_remote_copy(
            hn_send.at[dest], hn_buf.at[me], h_ss.at[dest], h_rs.at[me],
            device_id={"ep": dest}, device_id_type=MESH)

    lax.fori_loop(0, heads, group, 0)
    hn_buf[me] = hn_send[me]
    for step in range(1, n):
        source = lax.rem(me + step, n)
        recv(hn_buf, h_rs, source).wait_recv()
    w_copy.wait()
    for part in range(g):
        normed = jnp.concatenate(
            [hn_buf[h * g + lax.rem(part + me, g)] for h in range(heads)], axis=1)
        for t in range(n_tp):
            piece = out_ref.shape[2]
            out_ref[t, part * sub : (part + 1) * sub, :] = jnp.dot(
                normed, w_buf[:, t * piece : (t + 1) * piece], preferred_element_type=f32).astype(bf16)
    for step in range(1, n):
        dest = lax.rem(me + step, n)
        if step % g == 0:
            k_copy(dest).wait_send()
            v_copy(dest).wait_send()
        q_copy(dest).wait_send()
        hn_copy(dest).wait_send()
        tok_copy(dest).wait_send()
    for step in range(1, n_tp):
        other = lax.rem(my_tp + step, n_tp)
        spread_arrival(other).wait_recv()
        tok_spread(other).wait_send()
    for p in range(heads):
        for step in range(1, g):
            for copy in forward(p * g + my_core, step):
                copy.wait_send()


def g_cols(sub):
    return 2 * sub


def exchange_attention(query_pairs, key_pairs, value_rows, head_lambda, head_gain, out_weight, outgoing):
    n = lax.axis_size("ep")
    rows = query_pairs.shape[0]
    heads = head_lambda.shape[0]
    width = query_pairs.shape[1] // heads
    head_size = width // 2
    vw = value_rows.shape[1] // heads
    sub = rows * heads // n
    positions = lax.axis_index("ep") * rows + jnp.arange(rows, dtype=jnp.int32)
    half = head_size // 2
    frequency = theta_base ** (-(jnp.arange(half, dtype=f32) * 2.0) / head_size)
    angles = positions.astype(f32)[:, None] * frequency[None, :]
    cosine, sine = jnp.cos(angles), jnp.sin(angles)
    cosines = jnp.concatenate([cosine] * 4, axis=1)
    sines = jnp.concatenate([-sine, sine] * 2, axis=1)
    turned = jax.ShapeDtypeStruct((heads, rows, width), bf16)
    rq, rk = pl.pallas_call(
        functools.partial(rotate_kernel, head_size, head_size ** (-0.5)),
        out_shape=(turned, turned),
        name="rotate",
    )(query_pairs, key_pairs, cosines, sines)
    any_spec = pl.BlockSpec(memory_space=pl.ANY)
    vmem = pl.BlockSpec(memory_space=pltpu.VMEM)
    dma = pltpu.SemaphoreType.DMA
    g = n // heads
    n_tp = lax.axis_size("tp")
    return pl.pallas_call(
        functools.partial(attention_kernel, n, heads),
        out_shape=(
            jax.ShapeDtypeStruct((n_tp, rows, out_weight.shape[1] // n_tp), bf16),
            jax.ShapeDtypeStruct((n_tp,) + outgoing.shape, bf16),
        ),
        in_specs=[pl.BlockSpec(memory_space=pltpu.SMEM), vmem] + [any_spec] * 5,
        out_specs=(vmem, any_spec),
        scratch_shapes=[
            pltpu.VMEM((n, sub, width), bf16),
            pltpu.VMEM((n, rows, width), bf16),
            pltpu.VMEM((n, rows, vw), bf16),
            pltpu.VMEM((n, vw, rows), bf16),
            pltpu.VMEM((n, sub, vw), bf16),
            pltpu.VMEM((n, sub, vw), bf16),
            pltpu.VMEM(out_weight.shape, bf16),
            pltpu.VMEM((vw, 2 * sub), f32),
            pltpu.VMEM((1, 2 * sub), f32),
            pltpu.VMEM((1, 2 * sub), f32),
            dma((n,)), dma((n,)), dma((n,)), dma((n,)), dma((n,)), dma((n,)),
            dma((n, g)), dma((n,)), dma((n, g)), dma((n,)),
            dma((n,)), dma((n,)), dma((4,)), dma(()),
            dma((n,)), dma((n,)), dma((n_tp,)), dma((n_tp,)),
        ],
        compiler_params=pltpu.CompilerParams(
            collective_id=0, has_side_effects=True, vmem_limit_bytes=56 * 2**20),
        cost_estimate=pl.CostEstimate(flops=20 * 10**9, bytes_accessed=8 * 2**20, transcendentals=5 * 10**6),
        name="attention",
    )(head_lambda, head_gain.reshape(1, vw), rq, rk, value_rows, out_weight, outgoing)


def expert_kernel(
    n, n_tp, mix_ref, arr_ref, xn_ref, place_ref, rw_ref, wg_ref, wu_ref, wd_ref, sg_ref, su_ref, sd_ref,
    attn_ref, moe_ref,
    mix_in, arr, wg, wu, wd, sg, su, sd, sh_send, sh_in, ex_send, ex_in, y_buf, ret,
    loc, m_ss, m_rs, s_ss, s_rs, e_ss, e_rs, y_ss, y_rs,
):
    me = lax.axis_index("ep")
    my_tp = lax.axis_index("tp")
    piece = moe_ref.shape[1]
    cap = y_buf.shape[1]
    barrier = pltpu.get_barrier_semaphore()
    for step in range(1, n):
        pl.semaphore_signal(barrier, inc=1, device_id={"ep": lax.rem(me + step, n)}, device_id_type=MESH)
    for step in range(1, n_tp):
        pl.semaphore_signal(barrier, inc=1, device_id={"tp": lax.rem(my_tp + step, n_tp)}, device_id_type=MESH)
    loads = [
        pltpu.make_async_copy(source, target, loc.at[i])
        for i, (source, target) in enumerate((
            (sg_ref, sg), (su_ref, su), (sd_ref, sd), (arr_ref, arr),
            (wg_ref.at[0], wg), (wu_ref.at[0], wu), (wd_ref.at[0], wd),
            (mix_ref.at[my_tp], mix_in.at[my_tp])))
    ]
    for load in loads:
        load.start()
    pl.semaphore_wait(barrier, n - 1 + n_tp - 1)

    def scatter(send, into, send_sems, recv_sems, dest):
        return pltpu.make_async_remote_copy(
            send.at[dest], into.at[my_tp], send_sems.at[dest], recv_sems.at[my_tp],
            device_id={"tp": dest}, device_id_type=MESH)

    def arrival(into, recv_sems, source, axis):
        return pltpu.make_async_remote_copy(
            into.at[source], into.at[source], recv_sems.at[source], recv_sems.at[source],
            device_id={axis: lax.rem(lax.axis_index(axis) + 1, n if axis == "ep" else n_tp)},
            device_id_type=MESH)

    peers = [lax.rem(my_tp + step, n_tp) for step in (*range(1, n_tp), 0)]
    for dest in peers[:-1]:
        scatter(mix_ref, mix_in, m_ss, m_rs, dest).start()

    def columns(dest):
        return pl.ds(pl.multiple_of(dest * piece, piece), piece)

    def gated(gate, up):
        return (gate / (1.0 + jnp.exp(-gate)) * up).astype(bf16)

    for i in (0, 1, 2):
        loads[i].wait()
    xn = xn_ref[...]
    hidden = gated(
        jnp.dot(xn, sg[...], preferred_element_type=f32),
        jnp.dot(xn, su[...], preferred_element_type=f32))
    for dest in peers:
        sh_send[dest] = jnp.dot(hidden, sd[:, columns(dest)], preferred_element_type=f32).astype(bf16)
    for i in (3, 4, 5, 6):
        loads[i].wait()
    gate = up = None
    for t in range(n_tp):
        rows = arr[t].reshape(n * cap, piece)
        span = slice(t * piece, (t + 1) * piece)
        gate_part = jnp.dot(rows, wg[span, :], preferred_element_type=f32)
        up_part = jnp.dot(rows, wu[span, :], preferred_element_type=f32)
        gate = gate_part if gate is None else gate + gate_part
        up = up_part if up is None else up + up_part
    hidden = gated(gate, up)
    for dest in peers:
        ex_send[dest] = jnp.dot(hidden, wd[:, columns(dest)], preferred_element_type=f32).astype(bf16)
        if dest is not peers[-1]:
            scatter(ex_send, ex_in, e_ss, e_rs, dest).start()
    for dest in peers[:-1]:
        scatter(sh_send, sh_in, s_ss, s_rs, dest).start()
    loads[7].wait()
    for source in peers[:-1]:
        arrival(mix_in, m_rs, source, "tp").wait_recv()
    total = mix_in[0].astype(f32)
    for t in range(1, n_tp):
        total = total + mix_in[t].astype(f32)
    attn_ref[...] = total.astype(bf16)

    def y_copy(dest):
        return pltpu.make_async_remote_copy(
            y_buf.at[dest], ret.at[me], y_ss.at[dest], y_rs.at[me],
            device_id={"ep": dest}, device_id_type=MESH)

    y = ex_send[my_tp].astype(f32)
    for source in peers[:-1]:
        arrival(ex_in, e_rs, source, "tp").wait_recv()
        y = y + ex_in[source].astype(f32)
    y_buf[...] = y.astype(bf16).reshape(n, cap, piece)
    for step in range(1, n):
        y_copy(lax.rem(me + step, n)).start()
    ret[me] = y_buf[me]
    out = sh_send[my_tp].astype(f32)
    for source in peers[:-1]:
        arrival(sh_in, s_rs, source, "tp").wait_recv()
        out = out + sh_in[source].astype(f32)
    for step in range(1, n):
        arrival(ret, y_rs, lax.rem(me + step, n), "ep").wait_recv()
    returned = ret[...].reshape(n * cap, piece)
    for k in range(place_ref.shape[0]):
        out = out + rw_ref[:, k : k + 1] * jnp.dot(place_ref[k], returned, preferred_element_type=f32)
    moe_ref[...] = out.astype(bf16)
    for dest in peers[:-1]:
        scatter(mix_ref, mix_in, m_ss, m_rs, dest).wait_send()
        scatter(ex_send, ex_in, e_ss, e_rs, dest).wait_send()
        scatter(sh_send, sh_in, s_ss, s_rs, dest).wait_send()
    for step in range(1, n):
        y_copy(lax.rem(me + step, n)).wait_send()


def exchange_all(
    query_pairs, key_pairs, value_rows, head_lambda, head_gain, out_weight, normed, routes, route_weight,
    gate_weight, up_weight, down_weight, shared_gate, shared_up, shared_down,
):
    n, n_tp = lax.axis_size("ep"), lax.axis_size("tp")
    tokens, model = normed.shape
    piece = model // n_tp
    rows = query_pairs.shape[0]
    cap = -(-(tokens * TOP_K * 5 // (4 * n)) // 8) * 8
    onehot = (routes[:, :, None] == jnp.arange(n, dtype=jnp.int32)).astype(bf16)
    lower = jnp.tril(jnp.ones((tokens, tokens), bf16))
    ranks = jnp.dot(lower, jnp.sum(onehot, axis=1), preferred_element_type=f32) - 1.0
    slots = jnp.sum(onehot.astype(f32) * (ranks[:, None, :] + jnp.arange(n, dtype=f32) * cap), axis=-1)
    slots = slots.astype(jnp.int32).T
    place = (slots[:, :, None] == jnp.arange(n * cap, dtype=jnp.int32)).astype(bf16)
    part = lax.dynamic_slice_in_dim(normed, lax.axis_index("tp") * piece, piece, axis=1)
    outgoing = lax.dot_general(
        jnp.sum(place, axis=0), part, (((0,), (0,)), ((), ())), preferred_element_type=f32).astype(bf16)
    mix, arr = exchange_attention(
        query_pairs, key_pairs, value_rows, head_lambda, head_gain, out_weight, outgoing.reshape(n, cap, piece))
    any_spec = pl.BlockSpec(memory_space=pl.ANY)
    vmem = pl.BlockSpec(memory_space=pltpu.VMEM)
    dma = pltpu.SemaphoreType.DMA
    hidden, shared = gate_weight.shape[2], shared_gate.shape[1]
    return pl.pallas_call(
        functools.partial(expert_kernel, n, n_tp),
        out_shape=(
            jax.ShapeDtypeStruct((rows, piece), bf16),
            jax.ShapeDtypeStruct((tokens, piece), bf16),
        ),
        in_specs=[any_spec, any_spec, vmem, vmem, vmem] + [any_spec] * 6,
        out_specs=(vmem, vmem),
        scratch_shapes=[
            pltpu.VMEM((n_tp, rows, piece), bf16),
            pltpu.VMEM((n_tp, n, cap, piece), bf16),
            pltpu.VMEM((model, hidden), bf16),
            pltpu.VMEM((model, hidden), bf16),
            pltpu.VMEM((hidden, model), bf16),
            pltpu.VMEM((model, shared), bf16),
            pltpu.VMEM((model, shared), bf16),
            pltpu.VMEM((shared, model), bf16),
            pltpu.VMEM((n_tp, tokens, piece), bf16),
            pltpu.VMEM((n_tp, tokens, piece), bf16),
            pltpu.VMEM((n_tp, n * cap, piece), bf16),
            pltpu.VMEM((n_tp, n * cap, piece), bf16),
            pltpu.VMEM((n, cap, piece), bf16),
            pltpu.VMEM((n, cap, piece), bf16),
            dma((8,)), dma((n_tp,)), dma((n_tp,)), dma((n_tp,)), dma((n_tp,)), dma((n_tp,)), dma((n_tp,)),
            dma((n,)), dma((n,)),
        ],
        compiler_params=pltpu.CompilerParams(
            collective_id=1, has_side_effects=True, vmem_limit_bytes=60 * 2**20),
        cost_estimate=pl.CostEstimate(flops=10 * 10**9, bytes_accessed=16 * 2**20, transcendentals=5 * 10**5),
        name="experts",
    )(mix, arr, normed, place, route_weight, gate_weight, up_weight, down_weight, shared_gate, shared_up, shared_down)


def local(
    query_pairs,
    key_pairs,
    value_rows,
    head_lambda,
    head_gain,
    out_weight,
    moe_input,
    ffn_gain,
    routes,
    route_weight,
    gate_weight,
    up_weight,
    down_weight,
    shared_gate,
    shared_up,
    shared_down,
):
    n = lax.axis_size("ep")
    heads = head_lambda.shape[0]
    rows = query_pairs.shape[0]
    fits = n % heads == 0 and n // heads > 1 and (rows * heads) % (n * 64) == 0
    row_values = moe_input.astype(jnp.float32)
    inverse_norm = lax.rsqrt(jnp.mean(row_values * row_values, axis=-1, keepdims=True) + norm_eps)
    normed = (row_values * inverse_norm * ffn_gain).astype(jnp.bfloat16)
    if fits:
        return exchange_all(
            query_pairs, key_pairs, value_rows, head_lambda, head_gain, out_weight, normed, routes, route_weight,
            gate_weight, up_weight, down_weight, shared_gate, shared_up, shared_down,
        )
    attn_out = generic_attention(query_pairs, key_pairs, value_rows, head_lambda, head_gain, out_weight)
    token_rows = normed.shape[0]
    experts = lax.axis_size("ep")
    capacity = token_rows * TOP_K * 5 // (4 * experts)
    flat_routes = routes.reshape(-1)
    onehot = (flat_routes[:, None] == jnp.arange(experts, dtype=jnp.int32)).astype(jnp.int32)
    slot_rank = jnp.sum((jnp.cumsum(onehot, axis=0) - 1) * onehot, axis=-1)
    slot_index = flat_routes * capacity + slot_rank
    token_index = jnp.arange(token_rows * TOP_K, dtype=jnp.int32) // TOP_K
    slot_rows = (
        jnp.full((experts * capacity,), token_rows, jnp.int32).at[slot_index].set(token_index)
    )
    padded = jnp.concatenate([normed, jnp.zeros((1, normed.shape[1]), jnp.bfloat16)], axis=0)
    outgoing = padded[slot_rows]
    arrived = lax.all_to_all(outgoing, "ep", split_axis=0, concat_axis=0, tiled=True)
    gate_part = jnp.dot(arrived, gate_weight[0], preferred_element_type=jnp.float32)
    up_part = jnp.dot(arrived, up_weight[0], preferred_element_type=jnp.float32)
    hidden = (jax.nn.silu(gate_part) * up_part).astype(jnp.bfloat16)
    expert_terms = jnp.dot(hidden, down_weight[0], preferred_element_type=jnp.float32)
    shared_gated = jnp.dot(normed, shared_gate, preferred_element_type=jnp.float32)
    shared_lifted = jnp.dot(normed, shared_up, preferred_element_type=jnp.float32)
    shared_hidden = (jax.nn.silu(shared_gated) * shared_lifted).astype(jnp.bfloat16)
    shared_terms = jnp.dot(shared_hidden, shared_down, preferred_element_type=jnp.float32)
    expert_sum, shared_sum = (
        lax.psum_scatter(
            expert_terms.astype(jnp.bfloat16), "tp", scatter_dimension=1, tiled=True
        ).astype(jnp.float32),
        lax.psum_scatter(
            shared_terms.astype(jnp.bfloat16), "tp", scatter_dimension=1, tiled=True
        ).astype(jnp.float32),
    )
    returned = lax.all_to_all(
        expert_sum.astype(jnp.bfloat16), "ep", split_axis=0, concat_axis=0, tiled=True
    )
    picked = returned[slot_index.reshape(token_rows, TOP_K)]
    moe_out = (
        jnp.sum(route_weight[..., None] * picked.astype(jnp.float32), axis=1) + shared_sum
    ).astype(jnp.bfloat16)
    return (attn_out, moe_out)


def solution(mesh):
    return jax.shard_map(
        local,
        mesh=mesh,
        in_specs=(
            P("ep", "tp"),
            P("ep", "tp"),
            P("ep", "tp"),
            P("tp"),
            P(),
            P("tp", None),
            P("ep", None),
            P(),
            P("ep", None),
            P("ep", None),
            P("ep", None, "tp"),
            P("ep", None, "tp"),
            P("ep", "tp", None),
            P(None, "tp"),
            P(None, "tp"),
            P("tp", None),
        ),
        out_specs=(P("ep", "tp"), P("ep", "tp")),
        check_vma=False,
    )
```
